32 devices in a mesh: sp: 8 (over z, y), tp: 4 (over x, core).
Axes of the slice: x: 2, y: 2, z: 4, core: 2. Of those that a mesh axis runs over, the one named last changes fastest.
Arguments:
- stream: bfloat16 [2048, 2048], P('sp'), may hold values from -6 to 6
- attn_gain: float32 [2, 2048], replicated, may hold values from 0.1 to 1.9
- w_query: bfloat16 [2, 2048, 2048], P(None, None, 'tp'), may hold values from -0.125 to 0.125
- w_key: bfloat16 [2, 2048, 512], P(None, None, 'tp'), may hold values from -0.125 to 0.125
- w_value: bfloat16 [2, 2048, 512], P(None, None, 'tp'), may hold values from -0.125 to 0.125
- w_out: bfloat16 [2, 2048, 2048], P(None, 'tp'), may hold values from -1 to 1
- query_gain: float32 [2, 64], replicated, may hold values from 0.1 to 1.9
- key_gain: float32 [2, 64], replicated, may hold values from 0.1 to 1.9
- rel_bias: float32 [2, 32, 257], P(None, 'tp'), may hold values from -6 to 300
Outputs:
- result: bfloat16 [2048, 2048], P('sp', 'tp')
The draws below stay inside these ranges and needn't reach their ends.
All inputs are finite; a program needn't handle non-finite values.
Results may differ from the reference program's by a relative error of at most 0.02.
Values may be sent and summed in bfloat16 or wider, within the bound.
A program may use at most 64 MiB of HBM per device.

```python
import jax
import jax.numpy as jnp
from jax import lax

D = 2048
HEAD_DIM = 64
HEADS = 32
KV_HEADS = 8
SEG = 64
LEFT = 4
CLIP = 128
LAYERS = 2
TOKENS = 2048
N_TP = 4


def draw_rel_bias(key, part):
    subkeys = jax.random.split(jax.random.fold_in(key, 17), 1)
    shape = (LAYERS, HEADS, 2 * CLIP + 1)
    bias_table = jnp.clip(jax.random.normal(subkeys[0], shape, jnp.float32), -6.0, 6.0)
    return bias_table


def shard_levels(key, extent, cuts, least, high):
    level = 1.0
    for dim, parts in cuts:
        steps = jax.random.uniform(jax.random.fold_in(jax.random.fold_in(key, 6), dim), (parts,), jnp.float32, least / len(cuts), high / len(cuts))
        level = level * jnp.repeat(jnp.exp(steps), extent[dim] // parts).reshape((-1,) + (1,) * (len(extent) - 1 - dim))
    return level


def scatter_about(stream_key, extent, scale, bound, cuts=(), held_as=jnp.bfloat16):
    result = jax.random.normal(stream_key, extent, jnp.float32) * scale
    if len(cuts) > 0:
        result = shard_levels(stream_key, extent, cuts, -0.22, 0.18) * result
    return jnp.clip(result, min=-bound, max=bound).astype(held_as)


def setup_inputs(seed: int = 0) -> dict:
    arg_keys = jax.random.split(jax.random.key(seed), 10)
    return {
        "stream": scatter_about(arg_keys[0], (TOKENS, D), 1.0, 6.0, ((0, 8),)),
        "attn_gain": jnp.clip(1.0 + 0.18 * jax.random.normal(arg_keys[1], (LAYERS, D), jnp.float32), 0.1, 1.9),
        "w_query": scatter_about(arg_keys[2], (LAYERS, D, D), D ** -0.5, 0.125, ((2, 4),)),
        "w_key": scatter_about(arg_keys[3], (LAYERS, D, KV_HEADS * HEAD_DIM), D ** -0.5, 0.125, ((2, 4),)),
        "w_value": scatter_about(arg_keys[4], (LAYERS, D, KV_HEADS * HEAD_DIM), D ** -0.5, 0.125, ((2, 4),)),
        "w_out": scatter_about(arg_keys[5], (LAYERS, D, D), (D // 64) ** -0.5, 1.0, ((1, 4),)),
        "query_gain": jnp.clip(1.0 + 0.18 * jax.random.normal(arg_keys[6], (LAYERS, HEAD_DIM), jnp.float32), 0.1, 1.9),
        "key_gain": jnp.clip(1.0 + 0.18 * jax.random.normal(arg_keys[7], (LAYERS, HEAD_DIM), jnp.float32), 0.1, 1.9),
        "rel_bias": draw_rel_bias(jax.random.fold_in(arg_keys[9], 71), 0),
    }


norm_eps = 1e-06
masked_score = -1e+30

def rms_scale(values_in, gain):
    squared = lax.optimization_barrier(jnp.mean(values_in * values_in, axis=-1, keepdims=True))
    return values_in * lax.rsqrt(squared + norm_eps) * gain

def bias_block(bias_table, key_reach):
    query_pos = jnp.arange(key_reach, dtype=jnp.int32)[:, None]
    key_pos = jnp.arange(2 * key_reach, dtype=jnp.int32)[None, :]
    distance = jnp.clip(query_pos + key_reach - key_pos, -CLIP, CLIP) + CLIP
    return bias_table[:, distance].astype(jnp.float32)

def band_mask(key_reach, first_query):
    query_pos = jnp.arange(key_reach, dtype=jnp.int32)[:, None]
    key_pos = jnp.arange(2 * key_reach, dtype=jnp.int32)[None, :] - key_reach
    query_seg = query_pos // SEG
    key_seg = key_pos // SEG
    return (key_seg <= query_seg) & (key_seg >= query_seg - LEFT) & (first_query + key_pos >= 0)

def band_attention(queries, keys_all, values_all, bias_table):
    key_reach = LEFT * SEG
    group = HEADS // KV_HEADS
    total_rows = queries.shape[0]
    bias = bias_block(bias_table, key_reach).reshape(KV_HEADS, group, key_reach, 2 * key_reach)

    def one_block(block_index):
        start = block_index * key_reach
        query_rows = lax.dynamic_slice_in_dim(queries, start, key_reach, 0).reshape(key_reach, KV_HEADS, group, HEAD_DIM)
        key_rows = lax.dynamic_slice_in_dim(keys_all, start, 2 * key_reach, 0)
        value_rows = lax.dynamic_slice_in_dim(values_all, start, 2 * key_reach, 0)
        scores = jnp.einsum('qkgd,jkd->kgqj', query_rows.astype(jnp.float32), key_rows.astype(jnp.float32)) * HEAD_DIM ** (-0.5) + bias
        inside = band_mask(key_reach, start)
        scores = jnp.where(inside, scores, masked_score)
        peak = lax.optimization_barrier(jnp.max(scores, axis=-1, keepdims=True))
        expon = jnp.exp(scores - peak)
        weights = lax.optimization_barrier((expon / lax.optimization_barrier(jnp.sum(expon, axis=-1, keepdims=True))).astype(jnp.bfloat16))
        mixed = jnp.einsum('kgqj,jkd->qkgd', weights.astype(jnp.float32), value_rows.astype(jnp.float32))
        return mixed.astype(jnp.bfloat16).reshape(key_reach, HEADS * HEAD_DIM)
    blocks = lax.map(one_block, jnp.arange(total_rows // key_reach, dtype=jnp.int32))
    return blocks.reshape(total_rows, HEADS * HEAD_DIM)

def reference(stream, attn_gain, w_query, w_key, w_value, w_out, query_gain, key_gain, rel_bias):
    current = stream
    total_rows = stream.shape[0]
    key_reach = LEFT * SEG
    head_cols = D // N_TP
    for layer_index in range(LAYERS):
        normed = rms_scale(current.astype(jnp.float32), attn_gain[layer_index]).astype(jnp.bfloat16)
        query_flat = jnp.dot(normed, w_query[layer_index], preferred_element_type=jnp.float32)
        queries = rms_scale(query_flat.reshape(total_rows, HEADS, HEAD_DIM), query_gain[layer_index]).astype(jnp.bfloat16)
        key_flat = jnp.dot(normed, w_key[layer_index], preferred_element_type=jnp.float32)
        keys_now = rms_scale(key_flat.reshape(total_rows, KV_HEADS, HEAD_DIM), key_gain[layer_index]).astype(jnp.bfloat16)
        values_now = jnp.dot(normed, w_value[layer_index], preferred_element_type=jnp.float32).astype(jnp.bfloat16).reshape(total_rows, KV_HEADS, HEAD_DIM)
        padding = jnp.zeros((key_reach, KV_HEADS, HEAD_DIM), jnp.bfloat16)
        keys_all = jnp.concatenate([padding, keys_now], axis=0)
        values_all = jnp.concatenate([padding, values_now], axis=0)
        mixed = band_attention(queries, keys_all, values_all, rel_bias[layer_index])
        update = jnp.zeros((total_rows, D), jnp.float32)
        for group_index in range(N_TP):
            lower = group_index * head_cols
            partial_value = jnp.dot(mixed[:, lower:lower + head_cols], w_out[layer_index, lower:lower + head_cols], preferred_element_type=jnp.float32)
            update = update + lax.optimization_barrier(partial_value.astype(jnp.bfloat16)).astype(jnp.float32)
        current = (current.astype(jnp.float32) + update).astype(jnp.bfloat16)
    return current
```

```python
import functools

import jax
import jax.numpy as jnp
from jax import lax
from jax.experimental import pallas as pl
from jax.experimental.pallas import tpu as pltpu
from jax.sharding import PartitionSpec as P

HEAD_DIM = 64
SEG = 64
LEFT = 4
CLIP = 128
LAYERS = 2
SPAN = (LEFT + 1) * SEG
LINE = 384
LOG2E = 1.4426950408889634

norm_eps = 1e-06
masked_score = -1e30
F32 = jnp.float32
BF16 = jnp.bfloat16


def seg_rows(seg):
    return pl.ds(pl.multiple_of(seg * SEG, SEG), SEG)


def send(src, dst, send_sem, recv_sem, device):
    return pltpu.make_async_remote_copy(
        src_ref=src,
        dst_ref=dst,
        send_sem=send_sem,
        recv_sem=recv_sem,
        device_id=device,
        device_id_type=pl.DeviceIdType.MESH,
    )


def row_norm(x, gain):
    squared = jnp.mean(x * x, axis=-1, keepdims=True)
    return (x * lax.rsqrt(squared + norm_eps) * gain).astype(BF16)


def head_norm(x, gain_row, scale):
    width = x.shape[1]
    block = min(width, 256)
    row_head = lax.broadcasted_iota(jnp.int32, (block, block), 0) >> 6
    col_head = lax.broadcasted_iota(jnp.int32, (block, block), 1) >> 6
    spread = jnp.where(row_head == col_head, 1.0 / HEAD_DIM, 0.0).astype(BF16)
    gain = jnp.concatenate([gain_row] * (block // HEAD_DIM), axis=1) * scale
    outs = []
    for lower in range(0, width, block):
        part = x[:, lower : lower + block]
        squares = part * part
        high = squares.astype(BF16)
        low = (squares - high.astype(F32)).astype(BF16)
        mean = jnp.dot(high, spread, preferred_element_type=F32) + jnp.dot(
            low, spread, preferred_element_type=F32
        )
        outs.append((part * lax.rsqrt(mean + norm_eps) * gain).astype(BF16))
    return outs[0] if len(outs) == 1 else jnp.concatenate(outs, axis=1)


def body(
    n_sp, n_tp,
    stream, attn_gain_in, w_query, w_key, w_value, w_out, query_gain_in, key_gain_in, rel_bias_in,
    out,
    attn_gain, query_gain, key_gain, rel_bias,
    cur0, cur1, normed, wq, wk, wv, wo, queries, pair_made, halo, kdup, vdup, bias, ahead, mixed,
    psend, precv, own0, xsend, xrecv,
    psend1, precv1, own1, xsend1, xrecv1,
    w_sem, ps_sem, pr_sem, xs_sem, xr_sem, cs_sem, cr_sem, hs_sem, hr_sem,
    ps1_sem, xs1_sem, xr1_sem,
):
    row_count, width = cur0.shape
    segs = row_count // SEG
    q_width = wq.shape[2]
    kv_width = wk.shape[2]
    heads = q_width // HEAD_DIM
    kv_heads = kv_width // HEAD_DIM
    group = heads // kv_heads
    n_x = n_tp // 2
    feat = width // n_tp
    half_width = width // 2
    last = segs - 1
    me_sp = lax.axis_index("sp")
    me_tp = lax.axis_index("tp")
    core = lax.rem(me_tp, 2)
    chip = lax.div(me_tp, 2)
    partner = {"tp": chip * 2 + 1 - core}

    def chip_at(k):
        return lax.rem(chip + k, n_x)

    def peer(k):
        return {"tp": chip_at(k) * 2 + core}

    barrier = pltpu.get_barrier_semaphore()
    pl.semaphore_signal(barrier, inc=1, device_id=partner, device_id_type=pl.DeviceIdType.MESH)
    for k in range(1, n_x):
        pl.semaphore_signal(barrier, inc=1, device_id=peer(k), device_id_type=pl.DeviceIdType.MESH)

    @pl.when(me_sp > 0)
    def _():
        pl.semaphore_signal(
            barrier, inc=1, device_id={"sp": me_sp - 1}, device_id_type=pl.DeviceIdType.MESH
        )

    @pl.when(me_sp < n_sp - 1)
    def _():
        pl.semaphore_signal(
            barrier, inc=1, device_id={"sp": me_sp + 1}, device_id_type=pl.DeviceIdType.MESH
        )

    def load(n, src, dst):
        copy = pltpu.make_async_copy(src, dst, w_sem.at[n])
        copy.start()
        return copy

    early = pl.ds(last * SEG, SEG)
    late = pl.ds(0, last * SEG)
    early_load = load(0, stream.at[early], cur0.at[early])
    attn_gain_load = load(1, attn_gain_in, attn_gain)
    wk_load = load(2, w_key.at[0], wk.at[0])
    wv_load = load(3, w_value.at[0], wv.at[0])
    key_gain_load = load(4, key_gain_in, key_gain)
    late_load = load(5, stream.at[late], cur0.at[late])
    rel_bias_load = load(6, rel_bias_in, rel_bias)
    query_gain_load = load(7, query_gain_in, query_gain)
    wq_load = load(8, w_query.at[0], wq.at[0])
    wo_load = load(9, w_out.at[0], wo.at[0])

    low_half = lax.broadcasted_iota(jnp.int32, (SEG, 128), 1) < HEAD_DIM

    def build_bias(l):
        offset = lax.broadcasted_iota(jnp.int32, (2 * CLIP, LINE), 1)
        distance = jnp.clip(LEFT * SEG + SEG - 1 - offset, -CLIP, CLIP) + CLIP
        onehot = (lax.broadcasted_iota(jnp.int32, (2 * CLIP, LINE), 0) == distance).astype(F32)
        far = (distance[:1] == 2 * CLIP).astype(F32)
        table = rel_bias[l]
        line = jnp.dot(
            table[:, : 2 * CLIP], onehot, precision=lax.Precision.HIGHEST, preferred_element_type=F32
        ) + table[:, 2 * CLIP :] * far
        shut = jnp.where(me_sp == 0, masked_score, 0.0)
        shut_low = jnp.where(low_half, shut, 0.0)
        shut_high = jnp.where(low_half, 0.0, shut)
        for h in range(heads):
            spread = jnp.broadcast_to(line[h : h + 1], (SEG, LINE))
            turned = pltpu.roll(spread, LINE - (SEG - 1), 1, stride=1, stride_axis=0)
            moved = pltpu.roll(turned, LINE - SEG, 1)
            plain = [turned[:, n * 128 : (n + 1) * 128] for n in range(3)]
            other = [moved[:, n * 128 : (n + 1) * 128] for n in range(3)]

            def in_low(w):
                return other[w // 2] if w % 2 else plain[w // 2]

            def in_high(w):
                return plain[w // 2] if w % 2 else other[(w // 2 - 1) % 3]

            for seg in range(segs):
                own = LEFT - seg
                if l == 0 and seg == last:
                    order = list(range(own + 1, LEFT + 1)) + [own] + list(range(own))
                else:
                    order = [w for w in range(LEFT + 1) if w != own] + [own]
                tiles = []
                for n in range(3):
                    w = order[2 * n]
                    tile = in_low(w)
                    if n < 2:
                        v = order[2 * n + 1]
                        if in_high(v) is not tile:
                            tile = jnp.where(low_half, tile, in_high(v))
                        if w < own and v < own:
                            tile = tile + shut
                        elif w < own:
                            tile = tile + shut_low
                        elif v < own:
                            tile = tile + shut_high
                    else:
                        if w < own:
                            tile = tile + shut
                        tile = jnp.where(low_half, tile, masked_score)
                    tiles.append(tile)
                top = jnp.maximum(jnp.maximum(tiles[0], tiles[1]), tiles[2])
                peak = jnp.max(top, axis=-1, keepdims=True)
                for n in range(3):
                    bias[l, seg, h * SEG : (h + 1) * SEG, n * 128 : (n + 1) * 128] = (
                        tiles[n] - peak
                    ) * LOG2E

    for kv in range(kv_heads):
        vdup[kv, :, 128:] = jnp.ones((2 * row_count, 128), BF16)

    def keys_values(l, rows_in):
        both = jnp.concatenate([wk[l], wv[l]], axis=1)
        flat = jnp.dot(rows_in, both, preferred_element_type=F32)
        keys = head_norm(flat[:, :kv_width], key_gain[l : l + 1], 1.0)
        return keys, flat[:, kv_width:].astype(BF16)

    def make_queries(l, rows_in):
        flat = jnp.dot(rows_in, wq[l], preferred_element_type=F32)
        return head_norm(flat, query_gain[l : l + 1], HEAD_DIM ** (-0.5) * LOG2E)

    def place(seg):
        return row_count + lax.rem(seg + last, segs) * SEG

    def put_dup(keys, values, rows):
        for kv in range(kv_heads):
            cols = slice(kv * HEAD_DIM, (kv + 1) * HEAD_DIM)
            kdup[kv, rows, :] = jnp.concatenate([keys[:, cols]] * 2, axis=1)
            vdup[kv, rows, :128] = jnp.concatenate([values[:, cols]] * 2, axis=1)

    def halo_copy(l, seg):
        rows = seg_rows(seg)
        return send(
            pair_made.at[l, rows],
            halo.at[l, rows],
            hs_sem.at[l],
            hr_sem.at[l, seg],
            {"sp": lax.rem(me_sp + 1, n_sp)},
        )

    def start_halo(l, which):
        @pl.when(me_sp < n_sp - 1)
        def _():
            for seg in which:
                halo_copy(l, seg).start()

    def finish_halo(l, seg):
        @pl.when(me_sp > 0)
        def _():
            halo_copy(l, seg).wait_recv()
            got = halo[l, seg_rows(seg), :]
            put_dup(got[:, :kv_width], got[:, kv_width:], seg_rows(seg))

        @pl.when(me_sp == 0)
        def _():
            none = jnp.zeros((SEG, kv_width), BF16)
            put_dup(none, none, seg_rows(seg))

    main = LEFT * SEG
    tail_rows = pl.ds(2 * row_count - SEG, SEG)

    def attend_part(l, seg, kv, rows_at, lanes):
        rows = seg_rows(seg)
        stack = []
        for p in range(group // 2):
            lower = (kv * group + 2 * p) * HEAD_DIM
            tile = queries[rows, lower : lower + 128]
            none = jnp.zeros_like(tile)
            stack += [jnp.where(low_half, tile, none), jnp.where(low_half, none, tile)]
        stacked = jnp.concatenate(stack, axis=0)
        scores = lax.dot_general(
            stacked, kdup[kv, rows_at, :], (((1,), (1,)), ((), ())), preferred_element_type=F32
        )
        base = kv * group * SEG
        expon = jnp.exp2(scores + bias[l, seg, base : base + group * SEG, lanes]).astype(BF16)
        return jnp.dot(expon, vdup[kv, rows_at, :], preferred_element_type=F32)

    def put_mixed(kv, summed):
        for p in range(group // 2):
            lower = (kv * group + 2 * p) * HEAD_DIM
            even = summed[2 * p * SEG : (2 * p + 1) * SEG]
            odd = summed[(2 * p + 1) * SEG : (2 * p + 2) * SEG]
            top = jnp.where(low_half, even[:, :128], odd[:, :128])
            under = jnp.where(low_half, even[:, 128:], odd[:, 128:])
            mixed[:, lower : lower + 128] = (top / under).astype(BF16)

    def attend(l, seg):
        window = pl.ds(pl.multiple_of(seg * SEG, SEG), main)
        for kv in range(kv_heads):
            put_mixed(
                kv,
                attend_part(l, seg, kv, window, slice(0, main))
                + attend_part(l, seg, kv, tail_rows, slice(main, SPAN)),
            )

    def attend_ahead(l, rows_at):
        for kv in range(kv_heads):
            ahead[kv] = attend_part(l, last, kv, rows_at, slice(0, main))

    def attend_rest(l, rows_at):
        for kv in range(kv_heads):
            put_mixed(kv, ahead[kv] + attend_part(l, last, kv, rows_at, slice(main, SPAN)))

    def project_out(l, lower, size):
        cols = pl.ds(pl.multiple_of(lower, 128), size)
        return jnp.dot(mixed[...], wo[l, :, cols], preferred_element_type=F32)

    def meet():
        at_edge = jnp.logical_or(me_sp == 0, me_sp == n_sp - 1)

        @pl.when(at_edge)
        def _():
            pl.semaphore_wait(barrier, n_x + min(n_sp - 1, 1))

        @pl.when(jnp.logical_not(at_edge))
        def _():
            pl.semaphore_wait(barrier, n_x + 2)

    early_load.wait()
    attn_gain_load.wait()
    normed[early, :] = row_norm(cur0[early, :].astype(F32), attn_gain[0:1])
    wk_load.wait()
    wv_load.wait()
    key_gain_load.wait()
    keys, values = keys_values(0, normed[early, :])
    pair_made[0, early, :] = jnp.concatenate([keys, values], axis=1)
    meet()
    start_halo(0, [last])
    put_dup(keys, values, pl.ds(2 * row_count - 2 * SEG, SEG))
    late_load.wait()
    normed[late, :] = row_norm(cur0[late, :].astype(F32), attn_gain[0:1])
    keys, values = keys_values(0, normed[late, :])
    pair_made[0, late, :] = jnp.concatenate([keys, values], axis=1)
    start_halo(0, reversed(range(last)))
    put_dup(keys[:SEG], values[:SEG], tail_rows)
    put_dup(keys[SEG:], values[SEG:], pl.ds(row_count, (last - 1) * SEG))
    rel_bias_load.wait()
    query_gain_load.wait()
    wq_load.wait()
    queries[...] = make_queries(0, normed[...])
    build_bias(0)
    wo_load.wait()
    second_loads = [
        load(2, w_key.at[1], wk.at[1]),
        load(3, w_value.at[1], wv.at[1]),
        load(8, w_query.at[1], wq.at[1]),
        load(9, w_out.at[1], wo.at[1]),
    ]

    def partner_copy(i):
        return send(psend.at[i], precv.at[i], ps_sem.at[0], pr_sem.at[i], partner)

    def chip_copy(i, k):
        return send(
            xsend.at[i], xrecv.at[k - 1, i], xs_sem.at[k - 1], xr_sem.at[k - 1, i], peer(k)
        )

    my_half = pl.ds(pl.multiple_of(core * half_width, 128), half_width)

    def rows_copy(i, seg):
        rows = seg_rows(seg)
        return send(
            cur1.at[rows, my_half], cur1.at[rows, my_half], cs_sem.at[0], cr_sem.at[i], partner
        )

    out_step = min(half_width, 512)

    def first_out(i):
        for lower in range(0, half_width, out_step):
            psend[i, :, lower : lower + out_step] = project_out(
                0, (1 - core) * half_width + lower, out_step
            ).astype(BF16)
        partner_copy(i).start()
        for lower in range(0, half_width, out_step):
            own0[i, :, lower : lower + out_step] = project_out(
                0, core * half_width + lower, out_step
            )
        partner_copy(i).wait_recv()
        both = own0[i] + precv[i].astype(F32)
        own0[i] = both
        xsend[i] = both.astype(BF16)
        for k in range(1, n_x):
            chip_copy(i, k).start()

    attend_ahead(0, pl.ds(row_count, main))
    finish_halo(0, last)
    attend_rest(0, pl.ds(row_count - SEG, SEG))
    first_out(0)

    def first_round(i, carry):
        finish_halo(0, last - i)
        attend(0, last - i)
        first_out(i)
        return carry

    lax.fori_loop(1, segs, first_round, 0)
    build_bias(1)
    for copy in second_loads:
        copy.wait()

    def gather_rows(i, seg):
        rows = seg_rows(seg)
        total = own0[i]
        for k in range(1, n_x):
            chip_copy(i, k).wait_recv()
            total = total + xrecv[k - 1, i].astype(F32)
        cur1[rows, my_half] = (cur0[rows, my_half].astype(F32) + total).astype(BF16)
        rows_copy(i, seg).start()
        rows_copy(i, seg).wait_recv()
        normed[0:SEG, :] = row_norm(cur1[rows, :].astype(F32), attn_gain[1:2])
        return keys_values(1, normed[0:SEG, :])

    def second_queries(seg):
        queries[seg_rows(seg), :] = make_queries(1, normed[0:SEG, :])

    def put_own(keys, values, seg):
        pair_made[1, seg_rows(seg), :] = jnp.concatenate([keys, values], axis=1)
        start_halo(1, [seg])
        put_dup(keys, values, pl.ds(pl.multiple_of(place(seg), SEG), SEG))

    def second_round(i, carry):
        keys, values = gather_rows(i, last - i)
        second_queries(last - i)
        put_own(keys, values, last - i)
        return carry

    lax.fori_loop(0, last, second_round, 0)
    finish_halo(1, last)
    attend_ahead(1, pl.ds(row_count - SEG, main))
    keys, values = gather_rows(last, 0)
    put_own(keys, values, 0)

    def partner_copy1(s):
        return send(psend1.at[s], precv1.at[s], ps1_sem.at[0], pr_sem.at[s], partner)

    def chip_copy1(s, k):
        return send(
            xsend1.at[k - 1, s],
            xrecv1.at[k - 1, s],
            xs1_sem.at[k - 1],
            xr1_sem.at[k - 1, s],
            peer(k),
        )

    def last_partner(s):
        for k in range(n_x):
            lower = (chip_at(k) * 2 + 1 - core) * feat
            psend1[s, k] = project_out(1, lower, feat).astype(BF16)
        partner_copy1(s).start()

    def last_own(s):
        for k in range(n_x):
            lower = (chip_at(k) * 2 + core) * feat
            own1[s, k] = project_out(1, lower, feat)

    def last_sends(s):
        partner_copy1(s).wait_recv()
        for k in range(n_x):
            both = own1[s, k] + precv1[s, k].astype(F32)
            if k == 0:
                own1[s, k] = both
            else:
                xsend1[k - 1, s] = both.astype(BF16)
                chip_copy1(s, k).start()

    attend_rest(1, tail_rows)
    last_partner(0)
    second_queries(0)
    last_own(0)
    last_sends(0)

    def last_round(s, carry):
        finish_halo(1, last - s)
        attend(1, last - s)

        @pl.when(s > 1)
        def _():
            last_sends(s - 1)

        last_partner(s)
        last_own(s)
        return carry

    lax.fori_loop(1, segs, last_round, 0)
    last_sends(last)
    my_cols = pl.ds(pl.multiple_of(me_tp * feat, 128), feat)
    for s in range(segs):
        rows = slice((last - s) * SEG, (segs - s) * SEG)
        total = own1[s, 0]
        for k in range(1, n_x):
            chip_copy1(s, k).wait_recv()
            total = total + xrecv1[k - 1, s].astype(F32)
        out[rows, :] = (cur1[rows, my_cols].astype(F32) + total).astype(BF16)

    send(psend, precv, ps_sem.at[0], pr_sem.at[0], partner).wait_send()
    send(cur1.at[:, my_half], cur1.at[:, my_half], cs_sem.at[0], cr_sem.at[0], partner).wait_send()
    send(psend1, precv1, ps1_sem.at[0], pr_sem.at[0], partner).wait_send()
    for k in range(1, n_x):
        send(xsend, xrecv.at[k - 1], xs_sem.at[k - 1], xr_sem.at[k - 1, 0], peer(k)).wait_send()
        send(
            xsend1.at[k - 1], xrecv1.at[k - 1], xs1_sem.at[k - 1], xr1_sem.at[k - 1, 0], peer(k)
        ).wait_send()

    @pl.when(me_sp < n_sp - 1)
    def _():
        for l in range(LAYERS):
            send(
                pair_made.at[l], halo.at[l], hs_sem.at[l], hr_sem.at[l, 0],
                {"sp": lax.rem(me_sp + 1, n_sp)},
            ).wait_send()


def local(n_sp, n_tp, stream, attn_gain, w_query, w_key, w_value, w_out, query_gain, key_gain, rel_bias):
    row_count, width = stream.shape
    segs = row_count // SEG
    assert row_count == LEFT * SEG and n_tp % 2 == 0
    n_x = n_tp // 2
    feat = width // n_tp
    half_width = width // 2
    q_width = w_query.shape[2]
    kv_width = w_key.shape[2]
    kv_heads = kv_width // HEAD_DIM
    heads = q_width // HEAD_DIM
    group = heads // kv_heads
    others = max(n_x - 1, 1)
    dma = pltpu.SemaphoreType.DMA
    anyw = pl.BlockSpec(memory_space=pltpu.HBM)
    vmem = pl.BlockSpec(memory_space=pltpu.VMEM)
    scratch = [
        pltpu.VMEM(attn_gain.shape, F32),
        pltpu.VMEM(query_gain.shape, F32),
        pltpu.VMEM(key_gain.shape, F32),
        pltpu.VMEM(rel_bias.shape, F32),
        pltpu.VMEM((row_count, width), BF16),
        pltpu.VMEM((row_count, width), BF16),
        pltpu.VMEM((row_count, width), BF16),
        pltpu.VMEM(w_query.shape, BF16),
        pltpu.VMEM(w_key.shape, BF16),
        pltpu.VMEM(w_value.shape, BF16),
        pltpu.VMEM(w_out.shape, BF16),
        pltpu.VMEM((row_count, q_width), BF16),
        pltpu.VMEM((LAYERS, row_count, 2 * kv_width), BF16),
        pltpu.VMEM((LAYERS, row_count, 2 * kv_width), BF16),
        pltpu.VMEM((kv_heads, 2 * row_count, 128), BF16),
        pltpu.VMEM((kv_heads, 2 * row_count, 256), BF16),
        pltpu.VMEM((LAYERS, segs, heads * SEG, LINE), F32),
        pltpu.VMEM((kv_heads, group * SEG, 256), F32),
        pltpu.VMEM((SEG, q_width), BF16),
        pltpu.VMEM((segs, SEG, half_width), BF16),
        pltpu.VMEM((segs, SEG, half_width), BF16),
        pltpu.VMEM((segs, SEG, half_width), F32),
        pltpu.VMEM((segs, SEG, half_width), BF16),
        pltpu.VMEM((others, segs, SEG, half_width), BF16),
        pltpu.VMEM((segs, n_x, SEG, feat), BF16),
        pltpu.VMEM((segs, n_x, SEG, feat), BF16),
        pltpu.VMEM((segs, n_x, SEG, feat), F32),
        pltpu.VMEM((others, segs, SEG, feat), BF16),
        pltpu.VMEM((others, segs, SEG, feat), BF16),
        dma((10,)),
        dma((1,)), dma((segs,)),
        dma((others,)), dma((others, segs)),
        dma((1,)), dma((segs,)),
        dma((LAYERS,)), dma((LAYERS, segs)),
        dma((1,)),
        dma((others,)), dma((others, segs)),
    ]
    return pl.pallas_call(
        functools.partial(body, n_sp, n_tp),
        out_shape=pltpu.VMEM((row_count, feat), BF16),
        in_specs=[anyw] * 9,
        out_specs=vmem,
        scratch_shapes=scratch,
        compiler_params=pltpu.CompilerParams(
            collective_id=0, has_side_effects=True, vmem_limit_bytes=60 * 1024 * 1024
        ),
    )(stream, attn_gain, w_query, w_key, w_value, w_out, query_gain, key_gain, rel_bias)


def solution(mesh):
    return jax.shard_map(
        functools.partial(local, mesh.shape["sp"], mesh.shape["tp"]),
        mesh=mesh,
        in_specs=(
            P("sp", None),
            P(),
            P(None, None, "tp"),
            P(None, None, "tp"),
            P(None, None, "tp"),
            P(None, "tp", None),
            P(),
            P(),
            P(None, "tp", None),
        ),
        out_specs=P("sp", "tp"),
        check_vma=False,
    )
```

```python
import functools

import jax
import jax.numpy as jnp
from jax import lax
from jax.experimental import pallas as pl
from jax.experimental.pallas import tpu as pltpu
from jax.sharding import PartitionSpec as P

HEAD_DIM = 64
SEG = 64
LEFT = 4
CLIP = 128
LAYERS = 2
SPAN = (LEFT + 1) * SEG
LINE = 384
LOG2E = 1.4426950408889634

norm_eps = 1e-06
masked_score = -1e30
F32 = jnp.float32
BF16 = jnp.bfloat16


def seg_rows(seg):
    return pl.ds(pl.multiple_of(seg * SEG, SEG), SEG)


def send(src, dst, send_sem, recv_sem, device):
    return pltpu.make_async_remote_copy(
        src_ref=src,
        dst_ref=dst,
        send_sem=send_sem,
        recv_sem=recv_sem,
        device_id=device,
        device_id_type=pl.DeviceIdType.MESH,
    )


def row_norm(x, gain):
    squared = jnp.mean(x * x, axis=-1, keepdims=True)
    return (x * lax.rsqrt(squared + norm_eps) * gain).astype(BF16)


def head_norm(x, gain_row, scale):
    width = x.shape[1]
    block = min(width, 256)
    row_head = lax.broadcasted_iota(jnp.int32, (block, block), 0) >> 6
    col_head = lax.broadcasted_iota(jnp.int32, (block, block), 1) >> 6
    spread = jnp.where(row_head == col_head, 1.0 / HEAD_DIM, 0.0).astype(BF16)
    gain = jnp.concatenate([gain_row] * (block // HEAD_DIM), axis=1) * scale
    outs = []
    for lower in range(0, width, block):
        part = x[:, lower : lower + block]
        squares = part * part
        high = squares.astype(BF16)
        low = (squares - high.astype(F32)).astype(BF16)
        mean = jnp.dot(high, spread, preferred_element_type=F32) + jnp.dot(
            low, spread, preferred_element_type=F32
        )
        outs.append((part * lax.rsqrt(mean + norm_eps) * gain).astype(BF16))
    return outs[0] if len(outs) == 1 else jnp.concatenate(outs, axis=1)


def body(
    n_sp, n_tp,
    stream, attn_gain_in, w_query, w_key, w_value, w_out, query_gain_in, key_gain_in, rel_bias_in,
    out,
    attn_gain, query_gain, key_gain, rel_bias,
    cur0, cur1, normed, wq, wk, wv, wo, queries, pair_made, halo, kdup, vdup, line, bias, ahead, mixed,
    psend, precv, own0, xsend, xrecv,
    psend1, precv1, own1, xsend1, xrecv1,
    w_sem, ps_sem, pr_sem, xs_sem, xr_sem, cs_sem, cr_sem, hs_sem, hr_sem,
    ps1_sem, xs1_sem, xr1_sem,
):
    row_count, width = cur0.shape
    segs = row_count // SEG
    q_width = wq.shape[2]
    kv_width = wk.shape[2]
    heads = q_width // HEAD_DIM
    kv_heads = kv_width // HEAD_DIM
    group = heads // kv_heads
    n_x = n_tp // 2
    feat = width // n_tp
    half_width = width // 2
    last = segs - 1
    me_sp = lax.axis_index("sp")
    me_tp = lax.axis_index("tp")
    core = lax.rem(me_tp, 2)
    chip = lax.div(me_tp, 2)
    partner = {"tp": chip * 2 + 1 - core}

    def chip_at(k):
        return lax.rem(chip + k, n_x)

    def peer(k):
        return {"tp": chip_at(k) * 2 + core}

    barrier = pltpu.get_barrier_semaphore()
    pl.semaphore_signal(barrier, inc=1, device_id=partner, device_id_type=pl.DeviceIdType.MESH)
    for k in range(1, n_x):
        pl.semaphore_signal(barrier, inc=1, device_id=peer(k), device_id_type=pl.DeviceIdType.MESH)

    @pl.when(me_sp > 0)
    def _():
        pl.semaphore_signal(
            barrier, inc=1, device_id={"sp": me_sp - 1}, device_id_type=pl.DeviceIdType.MESH
        )

    @pl.when(me_sp < n_sp - 1)
    def _():
        pl.semaphore_signal(
            barrier, inc=1, device_id={"sp": me_sp + 1}, device_id_type=pl.DeviceIdType.MESH
        )

    def load(n, src, dst):
        copy = pltpu.make_async_copy(src, dst, w_sem.at[n])
        copy.start()
        return copy

    early = pl.ds(last * SEG, SEG)
    late = pl.ds(0, last * SEG)
    rel_bias_load = load(6, rel_bias_in, rel_bias)
    early_load = load(0, stream.at[early], cur0.at[early])
    attn_gain_load = load(1, attn_gain_in, attn_gain)
    wk_load = load(2, w_key.at[0], wk.at[0])
    wv_load = load(3, w_value.at[0], wv.at[0])
    key_gain_load = load(4, key_gain_in, key_gain)
    late_load = load(5, stream.at[late], cur0.at[late])
    query_gain_load = load(7, query_gain_in, query_gain)
    wq_load = load(8, w_query.at[0], wq.at[0])
    wo_load = load(9, w_out.at[0], wo.at[0])

    low_half = lax.broadcasted_iota(jnp.int32, (SEG, 128), 1) < HEAD_DIM

    def build_line():
        offset = lax.broadcasted_iota(jnp.int32, (2 * CLIP, LINE), 1)
        distance = jnp.clip(LEFT * SEG + SEG - 1 - offset, -CLIP, CLIP) + CLIP
        match = lax.broadcasted_iota(jnp.int32, (2 * CLIP, LINE), 0) == distance
        onehot = jnp.where(match, 1.0, 0.0).astype(BF16)
        far = (distance[:1] == 2 * CLIP).astype(F32)
        table = jnp.concatenate([rel_bias[l] for l in range(LAYERS)], axis=0)
        near = table[:, : 2 * CLIP]
        high = near.astype(BF16)
        near = near - high.astype(F32)
        middle = near.astype(BF16)
        low = (near - middle.astype(F32)).astype(BF16)
        high, middle, low = (
            jnp.dot(part, onehot, preferred_element_type=F32) for part in (high, middle, low)
        )
        line[...] = high + middle + low + table[:, 2 * CLIP :] * far

    def build_bias(l):
        shut = jnp.where(me_sp == 0, masked_score, 0.0)
        shut_low = jnp.where(low_half, shut, 0.0)
        shut_high = jnp.where(low_half, 0.0, shut)
        for h in range(heads):
            spread = jnp.broadcast_to(line[l * heads + h : l * heads + h + 1, :], (SEG, LINE))
            turned = pltpu.roll(spread, LINE - (SEG - 1), 1, stride=1, stride_axis=0)
            moved = pltpu.roll(turned, LINE - SEG, 1)
            plain = [turned[:, n * 128 : (n + 1) * 128] for n in range(3)]
            other = [moved[:, n * 128 : (n + 1) * 128] for n in range(3)]

            def in_low(w):
                return other[w // 2] if w % 2 else plain[w // 2]

            def in_high(w):
                return plain[w // 2] if w % 2 else other[(w // 2 - 1) % 3]

            for seg in range(segs):
                own = LEFT - seg
                if l == 0 and seg == last:
                    order = list(range(own + 1, LEFT + 1)) + [own] + list(range(own))
                else:
                    order = [w for w in range(LEFT + 1) if w != own] + [own]
                tiles = []
                for n in range(3):
                    w = order[2 * n]
                    tile = in_low(w)
                    if n < 2:
                        v = order[2 * n + 1]
                        if in_high(v) is not tile:
                            tile = jnp.where(low_half, tile, in_high(v))
                        if w < own and v < own:
                            tile = tile + shut
                        elif w < own:
                            tile = tile + shut_low
                        elif v < own:
                            tile = tile + shut_high
                    else:
                        if w < own:
                            tile = tile + shut
                        tile = jnp.where(low_half, tile, masked_score)
                    tiles.append(tile)
                top = jnp.maximum(jnp.maximum(tiles[0], tiles[1]), tiles[2])
                peak = jnp.max(top, axis=-1, keepdims=True)
                for n in range(3):
                    bias[l, seg, h * SEG : (h + 1) * SEG, n * 128 : (n + 1) * 128] = (
                        tiles[n] - peak
                    ) * LOG2E

    for kv in range(kv_heads):
        vdup[kv, :, 128:] = jnp.ones((2 * row_count, 128), BF16)

    def keys_values(l, rows_in):
        both = jnp.concatenate([wk[l], wv[l]], axis=1)
        flat = jnp.dot(rows_in, both, preferred_element_type=F32)
        keys = head_norm(flat[:, :kv_width], key_gain[l : l + 1], 1.0)
        return keys, flat[:, kv_width:].astype(BF16)

    def make_queries(l, rows_in):
        flat = jnp.dot(rows_in, wq[l], preferred_element_type=F32)
        return head_norm(flat, query_gain[l : l + 1], HEAD_DIM ** (-0.5) * LOG2E)

    def place(seg):
        return row_count + lax.rem(seg + last, segs) * SEG

    def put_dup(keys, values, rows):
        for kv in range(kv_heads):
            cols = slice(kv * HEAD_DIM, (kv + 1) * HEAD_DIM)
            kdup[kv, rows, :] = jnp.concatenate([keys[:, cols]] * 2, axis=1)
            vdup[kv, rows, :128] = jnp.concatenate([values[:, cols]] * 2, axis=1)

    def halo_copy(l, seg):
        rows = seg_rows(seg)
        return send(
            pair_made.at[l, rows],
            halo.at[l, rows],
            hs_sem.at[l],
            hr_sem.at[l, seg],
            {"sp": lax.rem(me_sp + 1, n_sp)},
        )

    def start_halo(l, which):
        @pl.when(me_sp < n_sp - 1)
        def _():
            for seg in which:
                halo_copy(l, seg).start()

    def finish_halo(l, seg):
        @pl.when(me_sp > 0)
        def _():
            halo_copy(l, seg).wait_recv()
            got = halo[l, seg_rows(seg), :]
            put_dup(got[:, :kv_width], got[:, kv_width:], seg_rows(seg))

        @pl.when(me_sp == 0)
        def _():
            none = jnp.zeros((SEG, kv_width), BF16)
            put_dup(none, none, seg_rows(seg))

    main = LEFT * SEG
    tail_rows = pl.ds(2 * row_count - SEG, SEG)

    def attend_part(l, seg, kv, rows_at, lanes):
        rows = seg_rows(seg)
        stack = []
        for p in range(group // 2):
            lower = (kv * group + 2 * p) * HEAD_DIM
            tile = queries[rows, lower : lower + 128]
            none = jnp.zeros_like(tile)
            stack += [jnp.where(low_half, tile, none), jnp.where(low_half, none, tile)]
        stacked = jnp.concatenate(stack, axis=0)
        scores = lax.dot_general(
            stacked, kdup[kv, rows_at, :], (((1,), (1,)), ((), ())), preferred_element_type=F32
        )
        base = kv * group * SEG
        expon = jnp.exp2(scores + bias[l, seg, base : base + group * SEG, lanes]).astype(BF16)
        return jnp.dot(expon, vdup[kv, rows_at, :], preferred_element_type=F32)

    def put_mixed(seg, kv, summed):
        rows = seg_rows(seg)
        for p in range(group // 2):
            lower = (kv * group + 2 * p) * HEAD_DIM
            even = summed[2 * p * SEG : (2 * p + 1) * SEG]
            odd = summed[(2 * p + 1) * SEG : (2 * p + 2) * SEG]
            top = jnp.where(low_half, even[:, :128], odd[:, :128])
            under = jnp.where(low_half, even[:, 128:], odd[:, 128:])
            mixed[rows, lower : lower + 128] = (top / under).astype(BF16)

    def attend(l, seg):
        window = pl.ds(pl.multiple_of(seg * SEG, SEG), main)
        for kv in range(kv_heads):
            put_mixed(
                seg,
                kv,
                attend_part(l, seg, kv, window, slice(0, main))
                + attend_part(l, seg, kv, tail_rows, slice(main, SPAN)),
            )

    def attend_ahead(l, seg, rows_at):
        for kv in range(kv_heads):
            ahead[last - seg, kv] = attend_part(l, seg, kv, rows_at, slice(0, main))

    def attend_rest(l, seg, rows_at):
        for kv in range(kv_heads):
            rest = attend_part(l, seg, kv, rows_at, slice(main, SPAN))
            put_mixed(seg, kv, ahead[last - seg, kv] + rest)

    def project_out(l, rows, lower, size):
        cols = pl.ds(pl.multiple_of(lower, 128), size)
        return jnp.dot(mixed[rows, :], wo[l, :, cols], preferred_element_type=F32)

    def meet():
        at_edge = jnp.logical_or(me_sp == 0, me_sp == n_sp - 1)

        @pl.when(at_edge)
        def _():
            pl.semaphore_wait(barrier, n_x + min(n_sp - 1, 1))

        @pl.when(jnp.logical_not(at_edge))
        def _():
            pl.semaphore_wait(barrier, n_x + 2)

    rel_bias_load.wait()
    early_load.wait()
    attn_gain_load.wait()
    build_line()
    normed[early, :] = row_norm(cur0[early, :].astype(F32), attn_gain[0:1])
    wk_load.wait()
    wv_load.wait()
    key_gain_load.wait()
    keys, values = keys_values(0, normed[early, :])
    pair_made[0, early, :] = jnp.concatenate([keys, values], axis=1)
    meet()
    start_halo(0, [last])
    put_dup(keys, values, pl.ds(2 * row_count - 2 * SEG, SEG))
    late_load.wait()
    normed[late, :] = row_norm(cur0[late, :].astype(F32), attn_gain[0:1])
    keys, values = keys_values(0, normed[late, :])
    pair_made[0, late, :] = jnp.concatenate([keys, values], axis=1)
    start_halo(0, reversed(range(last)))
    put_dup(keys[:SEG], values[:SEG], tail_rows)
    put_dup(keys[SEG:], values[SEG:], pl.ds(row_count, (last - 1) * SEG))
    query_gain_load.wait()
    wq_load.wait()
    wo_load.wait()
    queries[...] = make_queries(0, normed[...])
    build_bias(0)
    second_loads = [
        load(2, w_key.at[1], wk.at[1]),
        load(3, w_value.at[1], wv.at[1]),
        load(8, w_query.at[1], wq.at[1]),
        load(9, w_out.at[1], wo.at[1]),
    ]

    def partner_copy(i):
        return send(psend.at[i], precv.at[i], ps_sem.at[0], pr_sem.at[i], partner)

    def chip_copy(i, k):
        return send(
            xsend.at[i], xrecv.at[k - 1, i], xs_sem.at[k - 1], xr_sem.at[k - 1, i], peer(k)
        )

    my_half = pl.ds(pl.multiple_of(core * half_width, 128), half_width)

    def rows_copy(i, seg):
        rows = seg_rows(seg)
        return send(
            cur1.at[rows, my_half], cur1.at[rows, my_half], cs_sem.at[0], cr_sem.at[i], partner
        )

    out_step = min(half_width, 512)

    def first_partner(i):
        for lower in range(0, half_width, out_step):
            psend[i, :, lower : lower + out_step] = project_out(
                0, seg_rows(last - i), (1 - core) * half_width + lower, out_step
            ).astype(BF16)
        partner_copy(i).start()

    def first_own(i):
        for lower in range(0, half_width, out_step):
            own0[i, :, lower : lower + out_step] = project_out(
                0, seg_rows(last - i), core * half_width + lower, out_step
            )

    def first_sends(i):
        partner_copy(i).wait_recv()
        both = own0[i] + precv[i].astype(F32)
        own0[i] = both
        xsend[i] = both.astype(BF16)
        for k in range(1, n_x):
            chip_copy(i, k).start()

    attend_ahead(0, last, pl.ds(row_count, main))
    finish_halo(0, last)
    attend_rest(0, last, pl.ds(row_count - SEG, SEG))
    first_partner(0)
    first_own(0)
    first_sends(0)

    def first_round(i, carry):
        finish_halo(0, last - i)
        attend(0, last - i)
        first_partner(i)

        @pl.when(i > 1)
        def _():
            first_sends(i - 1)

        first_own(i)
        return carry

    lax.fori_loop(1, segs, first_round, 0)
    first_sends(last)

    def gather_rows(i, seg):
        rows = seg_rows(seg)
        total = own0[i]
        for k in range(1, n_x):
            chip_copy(i, k).wait_recv()
            total = total + xrecv[k - 1, i].astype(F32)
        cur1[rows, my_half] = (cur0[rows, my_half].astype(F32) + total).astype(BF16)
        rows_copy(i, seg).start()

    def second_keys(i, seg):
        rows = seg_rows(seg)
        rows_copy(i, seg).wait_recv()
        normed[rows, :] = row_norm(cur1[rows, :].astype(F32), attn_gain[1:2])
        keys, values = keys_values(1, normed[rows, :])
        pair_made[1, rows, :] = jnp.concatenate([keys, values], axis=1)
        start_halo(1, [seg])
        put_dup(keys, values, pl.ds(pl.multiple_of(place(seg), SEG), SEG))

    def second_queries(seg):
        queries[seg_rows(seg), :] = make_queries(1, normed[seg_rows(seg), :])

    gather_rows(0, last)
    build_bias(1)
    for copy in second_loads:
        copy.wait()
    second_keys(0, last)

    def second_round(i, carry):
        gather_rows(i, last - i)
        second_queries(segs - i)
        second_keys(i, last - i)
        return carry

    lax.fori_loop(1, last, second_round, 0)
    second_queries(1)
    gather_rows(last, 0)
    early_segs = (last, last - 1)
    for seg in early_segs:
        finish_halo(1, seg)
        attend_ahead(1, seg, pl.ds(seg * SEG, main))
    second_keys(last, 0)

    groups = (pl.ds((last - 1) * SEG, 2 * SEG),) + tuple(
        pl.ds(seg * SEG, SEG) for seg in reversed(range(last - 1))
    )

    def partner_copy1(g, k):
        rows = groups[g]
        return send(
            psend1.at[k, rows], precv1.at[k, rows], ps1_sem.at[0], pr_sem.at[g * n_x + k], partner
        )

    def chip_copy1(g, k):
        rows = groups[g]
        return send(
            xsend1.at[k - 1, rows],
            xrecv1.at[k - 1, rows],
            xs1_sem.at[k - 1],
            xr1_sem.at[k - 1, g],
            peer(k),
        )

    far_first = list(range(1, n_x)) + [0]

    def last_partner(g):
        for k in far_first:
            lower = (chip_at(k) * 2 + 1 - core) * feat
            psend1[k, groups[g], :] = project_out(1, groups[g], lower, feat).astype(BF16)
            partner_copy1(g, k).start()

    def last_own(g):
        for k in far_first:
            lower = (chip_at(k) * 2 + core) * feat
            own1[k, groups[g], :] = project_out(1, groups[g], lower, feat)

    def last_sends(g):
        for k in range(1, n_x):
            partner_copy1(g, k).wait_recv()
            both = own1[k, groups[g], :] + precv1[k, groups[g], :].astype(F32)
            xsend1[k - 1, groups[g], :] = both.astype(BF16)
            chip_copy1(g, k).start()

    for seg in early_segs:
        attend_rest(1, seg, tail_rows)
    last_partner(0)
    second_queries(0)
    last_own(0)
    last_sends(0)
    for g in range(1, len(groups)):
        finish_halo(1, last - 1 - g)
        attend(1, last - 1 - g)
        if g > 1:
            last_sends(g - 1)
        last_partner(g)
        last_own(g)
    last_sends(len(groups) - 1)
    my_cols = pl.ds(pl.multiple_of(me_tp * feat, 128), feat)
    for g in range(len(groups)):
        rows = groups[g]
        partner_copy1(g, 0).wait_recv()
        total = cur1[rows, my_cols].astype(F32) + own1[0, rows, :] + precv1[0, rows, :].astype(F32)
        for k in range(1, n_x):
            chip_copy1(g, k).wait_recv()
            total = total + xrecv1[k - 1, rows, :].astype(F32)
        out[rows, :] = total.astype(BF16)

    send(psend, precv, ps_sem.at[0], pr_sem.at[0], partner).wait_send()
    send(cur1.at[:, my_half], cur1.at[:, my_half], cs_sem.at[0], cr_sem.at[0], partner).wait_send()
    send(psend1, precv1, ps1_sem.at[0], pr_sem.at[0], partner).wait_send()
    for k in range(1, n_x):
        send(xsend, xrecv.at[k - 1], xs_sem.at[k - 1], xr_sem.at[k - 1, 0], peer(k)).wait_send()
        send(
            xsend1.at[k - 1], xrecv1.at[k - 1], xs1_sem.at[k - 1], xr1_sem.at[k - 1, 0], peer(k)
        ).wait_send()

    @pl.when(me_sp < n_sp - 1)
    def _():
        for l in range(LAYERS):
            send(
                pair_made.at[l], halo.at[l], hs_sem.at[l], hr_sem.at[l, 0],
                {"sp": lax.rem(me_sp + 1, n_sp)},
            ).wait_send()


def local(n_sp, n_tp, stream, attn_gain, w_query, w_key, w_value, w_out, query_gain, key_gain, rel_bias):
    row_count, width = stream.shape
    segs = row_count // SEG
    assert row_count == LEFT * SEG and n_tp % 2 == 0
    n_x = n_tp // 2
    feat = width // n_tp
    half_width = width // 2
    q_width = w_query.shape[2]
    kv_width = w_key.shape[2]
    kv_heads = kv_width // HEAD_DIM
    heads = q_width // HEAD_DIM
    group = heads // kv_heads
    others = max(n_x - 1, 1)
    dma = pltpu.SemaphoreType.DMA
    anyw = pl.BlockSpec(memory_space=pltpu.HBM)
    vmem = pl.BlockSpec(memory_space=pltpu.VMEM)
    scratch = [
        pltpu.VMEM(attn_gain.shape, F32),
        pltpu.VMEM(query_gain.shape, F32),
        pltpu.VMEM(key_gain.shape, F32),
        pltpu.VMEM(rel_bias.shape, F32),
        pltpu.VMEM((row_count, width), BF16),
        pltpu.VMEM((row_count, width), BF16),
        pltpu.VMEM((row_count, width), BF16),
        pltpu.VMEM(w_query.shape, BF16),
        pltpu.VMEM(w_key.shape, BF16),
        pltpu.VMEM(w_value.shape, BF16),
        pltpu.VMEM(w_out.shape, BF16),
        pltpu.VMEM((row_count, q_width), BF16),
        pltpu.VMEM((LAYERS, row_count, 2 * kv_width), BF16),
        pltpu.VMEM((LAYERS, row_count, 2 * kv_width), BF16),
        pltpu.VMEM((kv_heads, 2 * row_count, 128), BF16),
        pltpu.VMEM((kv_heads, 2 * row_count, 256), BF16),
        pltpu.VMEM((LAYERS * heads, LINE), F32),
        pltpu.VMEM((LAYERS, segs, heads * SEG, LINE), F32),
        pltpu.VMEM((2, kv_heads, group * SEG, 256), F32),
        pltpu.VMEM((row_count, q_width), BF16),
        pltpu.VMEM((segs, SEG, half_width), BF16),
        pltpu.VMEM((segs, SEG, half_width), BF16),
        pltpu.VMEM((segs, SEG, half_width), F32),
        pltpu.VMEM((segs, SEG, half_width), BF16),
        pltpu.VMEM((others, segs, SEG, half_width), BF16),
        pltpu.VMEM((n_x, row_count, feat), BF16),
        pltpu.VMEM((n_x, row_count, feat), BF16),
        pltpu.VMEM((n_x, row_count, feat), F32),
        pltpu.VMEM((others, row_count, feat), BF16),
        pltpu.VMEM((others, row_count, feat), BF16),
        dma((10,)),
        dma((1,)), dma((max(segs, (segs - 1) * n_x),)),
        dma((others,)), dma((others, segs)),
        dma((1,)), dma((segs,)),
        dma((LAYERS,)), dma((LAYERS, segs)),
        dma((1,)),
        dma((others,)), dma((others, segs - 1)),
    ]
    return pl.pallas_call(
        functools.partial(body, n_sp, n_tp),
        out_shape=pltpu.VMEM((row_count, feat), BF16),
        in_specs=[anyw] * 9,
        out_specs=vmem,
        scratch_shapes=scratch,
        compiler_params=pltpu.CompilerParams(
            collective_id=0, has_side_effects=True, vmem_limit_bytes=60 * 1024 * 1024
        ),
    )(stream, attn_gain, w_query, w_key, w_value, w_out, query_gain, key_gain, rel_bias)


def solution(mesh):
    return jax.shard_map(
        functools.partial(local, mesh.shape["sp"], mesh.shape["tp"]),
        mesh=mesh,
        in_specs=(
            P("sp", None),
            P(),
            P(None, None, "tp"),
            P(None, None, "tp"),
            P(None, None, "tp"),
            P(None, "tp", None),
            P(),
            P(),
            P(None, "tp", None),
        ),
        out_specs=P("sp", "tp"),
        check_vma=False,
    )
```

```python
import functools

import jax
import jax.numpy as jnp
from jax import lax
from jax.experimental import pallas as pl
from jax.experimental.pallas import tpu as pltpu
from jax.sharding import PartitionSpec as P

HEAD_DIM = 64
SEG = 64
LEFT = 4
CLIP = 128
LAYERS = 2
SPAN = (LEFT + 1) * SEG
LINE = 384
LOG2E = 1.4426950408889634

norm_eps = 1e-06
masked_score = -1e30
F32 = jnp.float32
BF16 = jnp.bfloat16


def seg_rows(seg):
    return pl.ds(pl.multiple_of(seg * SEG, SEG), SEG)


def send(src, dst, send_sem, recv_sem, device):
    return pltpu.make_async_remote_copy(
        src_ref=src,
        dst_ref=dst,
        send_sem=send_sem,
        recv_sem=recv_sem,
        device_id=device,
        device_id_type=pl.DeviceIdType.MESH,
    )


def row_squares(x):
    return jnp.sum(x * x, axis=-1, keepdims=True)


def row_scale(squares, width):
    scale = lax.rsqrt(squares * (1.0 / width) + norm_eps)
    return jnp.broadcast_to(scale, (squares.shape[0], 128))


def widen(scale, width):
    return jnp.concatenate([scale] * -(-width // 128), axis=1)[:, :width]


def head_norm(x, row_scales, gain_row, scale):
    width = x.shape[1]
    x = x * widen(row_scales, width)
    block = min(width, 256)
    row_head = lax.broadcasted_iota(jnp.int32, (block, block), 0) >> 6
    col_head = lax.broadcasted_iota(jnp.int32, (block, block), 1) >> 6
    spread = jnp.where(row_head == col_head, 1.0 / HEAD_DIM, 0.0).astype(BF16)
    gain = jnp.concatenate([gain_row] * (block // HEAD_DIM), axis=1) * scale
    outs = []
    for lower in range(0, width, block):
        part = x[:, lower : lower + block]
        mean = jnp.dot((part * part).astype(BF16), spread, preferred_element_type=F32)
        outs.append((part * lax.rsqrt(mean + norm_eps) * gain).astype(BF16))
    return outs[0] if len(outs) == 1 else jnp.concatenate(outs, axis=1)


def body(
    n_sp, n_tp,
    stream, attn_gain_in, w_query, w_key, w_value, w_out, query_gain_in, key_gain_in, rel_bias_in,
    out,
    attn_gain, query_gain, key_gain, rel_bias,
    cur0, cur1, gained, scales, wq, wkv, wo, queries, pair_made, halo, kdup, vdup, line, bias, ahead, mixed,
    psend, precv, own0, xsend, xrecv,
    psend1, precv1, own1, xsend1, xrecv1,
    w_sem, ps_sem, pr_sem, xs_sem, xr_sem, cs_sem, cr_sem, hs_sem, hr_sem,
    ps1_sem, xs1_sem, xr1_sem,
):
    row_count, width = cur0.shape
    segs = row_count // SEG
    q_width = wq.shape[2]
    kv_width = w_key.shape[2]
    heads = q_width // HEAD_DIM
    kv_heads = kv_width // HEAD_DIM
    group = heads // kv_heads
    n_x = n_tp // 2
    feat = width // n_tp
    half_width = width // 2
    last = segs - 1
    me_sp = lax.axis_index("sp")
    me_tp = lax.axis_index("tp")
    core = lax.rem(me_tp, 2)
    chip = lax.div(me_tp, 2)
    partner = {"tp": chip * 2 + 1 - core}

    def chip_at(k):
        return lax.rem(chip + k, n_x)

    def core_at(k):
        return lax.rem(core + k, 2)

    def peer(k):
        return {"tp": chip_at(k) * 2 + core_at(k)}

    my_part = lax.rem(core + chip, 2)

    barrier = pltpu.get_barrier_semaphore()
    pl.semaphore_signal(barrier, inc=1, device_id=partner, device_id_type=pl.DeviceIdType.MESH)
    for k in range(1, n_x):
        pl.semaphore_signal(barrier, inc=1, device_id=peer(k), device_id_type=pl.DeviceIdType.MESH)

    @pl.when(me_sp > 0)
    def _():
        pl.semaphore_signal(
            barrier, inc=1, device_id={"sp": me_sp - 1}, device_id_type=pl.DeviceIdType.MESH
        )

    @pl.when(me_sp < n_sp - 1)
    def _():
        pl.semaphore_signal(
            barrier, inc=1, device_id={"sp": me_sp + 1}, device_id_type=pl.DeviceIdType.MESH
        )

    def load(n, src, dst):
        copy = pltpu.make_async_copy(src, dst, w_sem.at[n])
        copy.start()
        return copy

    early = pl.ds(last * SEG, SEG)
    late = pl.ds(0, last * SEG)
    early_load = load(0, stream.at[early], cur0.at[early])
    attn_gain_load = load(1, attn_gain_in, attn_gain)
    joined = kv_width % 128 == 0

    def kv_part(l, n):
        if joined:
            return wkv.at[l, :, pl.ds(n * kv_width, kv_width)]
        return wkv.at[l, n]

    wk_load = load(2, w_key.at[0], kv_part(0, 0))
    wv_load = load(3, w_value.at[0], kv_part(0, 1))
    key_gain_load = load(4, key_gain_in, key_gain)
    late_load = load(5, stream.at[late], cur0.at[late])
    rel_bias_load = load(6, rel_bias_in, rel_bias)
    query_gain_load = load(7, query_gain_in, query_gain)
    wq_load = load(8, w_query.at[0], wq.at[0])
    wo_load = load(9, w_out.at[0], wo.at[0])

    low_half = lax.broadcasted_iota(jnp.int32, (SEG, 128), 1) < HEAD_DIM

    def build_line():
        offset = lax.broadcasted_iota(jnp.int32, (2 * CLIP, LINE), 1)
        distance = jnp.clip(LEFT * SEG + SEG - 1 - offset, -CLIP, CLIP) + CLIP
        match = lax.broadcasted_iota(jnp.int32, (2 * CLIP, LINE), 0) == distance
        onehot = jnp.where(match, 1.0, 0.0).astype(BF16)
        far = (distance[:1] == 2 * CLIP).astype(F32)
        table = jnp.concatenate([rel_bias[l] for l in range(LAYERS)], axis=0)
        near = table[:, : 2 * CLIP]
        high = near.astype(BF16)
        near = near - high.astype(F32)
        middle = near.astype(BF16)
        low = (near - middle.astype(F32)).astype(BF16)
        high, middle, low = (
            jnp.dot(part, onehot, preferred_element_type=F32) for part in (high, middle, low)
        )
        line[...] = (high + middle + low + table[:, 2 * CLIP :] * far) * LOG2E

    def build_bias(l):
        for h in range(heads):
            row = slice(l * heads + h, l * heads + h + 1)
            spread = jnp.broadcast_to(line[row, 128:], (SEG, LINE - 128))
            turned = pltpu.roll(spread, LINE - 128 - (SEG - 1), 1, stride=1, stride_axis=0)
            tiles = [
                jnp.broadcast_to(line[row, :128], (SEG, 128)),
                turned[:, :128],
                jnp.where(low_half, turned[:, 128:], masked_score),
            ]
            top = jnp.maximum(jnp.maximum(tiles[0], tiles[1]), tiles[2])
            peak = jnp.max(top, axis=-1, keepdims=True)
            for n in range(3):
                bias[l, 2, h * SEG : (h + 1) * SEG, n * 128 : (n + 1) * 128] = tiles[n] - peak

    def build_edge(l):
        @pl.when(me_sp == 0)
        def _():
            for h in range(heads):
                rows = slice(h * SEG, (h + 1) * SEG)
                near = bias[l, 2, rows, 256:]
                middle = jnp.where(low_half, masked_score, bias[l, 2, rows, 128:256])
                shut = jnp.full((SEG, 128), masked_score, F32)
                peak = jnp.max(near, axis=-1, keepdims=True)
                bias[l, 0, rows, :128] = shut
                bias[l, 0, rows, 128:256] = shut
                bias[l, 0, rows, 256:] = near - peak
                peak = jnp.maximum(peak, jnp.max(middle, axis=-1, keepdims=True))
                bias[l, 1, rows, :128] = shut
                bias[l, 1, rows, 128:256] = middle - peak
                bias[l, 1, rows, 256:] = near - peak

    for kv in range(kv_heads):
        vdup[kv, :, 128:] = jnp.ones((2 * row_count, 128), BF16)

    def take_rows(l, current, rows):
        x = current[rows, :].astype(F32)
        gained[rows, :] = (x * attn_gain[l : l + 1]).astype(BF16)
        scales[rows, :] = row_scale(row_squares(x), width)

    halves = [pl.ds(n * half_width, half_width) for n in range(2)]

    def half_dot(l, rows, half):
        if joined:
            both = wkv[l, half, :]
        else:
            both = jnp.concatenate([wkv[l, 0, half, :], wkv[l, 1, half, :]], axis=1)
        return jnp.dot(gained[rows, half], both, preferred_element_type=F32)

    def keys_values(l, rows):
        flat = half_dot(l, rows, halves[0]) + half_dot(l, rows, halves[1])
        return split_keys(l, rows, flat)

    def split_keys(l, rows, flat):
        keys = head_norm(flat[:, :kv_width], scales[rows, :], key_gain[l : l + 1], 1.0)
        values = flat[:, kv_width:] * widen(scales[rows, :], kv_width)
        return keys, values.astype(BF16)

    def make_queries(l, rows):
        flat = jnp.dot(gained[rows, :], wq[l], preferred_element_type=F32)
        queries[rows, :] = head_norm(
            flat, scales[rows, :], query_gain[l : l + 1], HEAD_DIM ** (-0.5) * LOG2E
        )

    def put_dup(keys, values, rows):
        for kv in range(kv_heads):
            cols = slice(kv * HEAD_DIM, (kv + 1) * HEAD_DIM)
            kdup[kv, rows, :] = jnp.concatenate([keys[:, cols]] * 2, axis=1)
            vdup[kv, rows, :128] = jnp.concatenate([values[:, cols]] * 2, axis=1)

    def halo_copy(l, rows, n):
        return send(
            pair_made.at[l, rows],
            halo.at[l, rows],
            hs_sem.at[l],
            hr_sem.at[n],
            {"sp": lax.rem(me_sp + 1, n_sp)},
        )

    def start_halo(l, rows, n, here=True):
        @pl.when(jnp.logical_and(me_sp < n_sp - 1, here))
        def _():
            halo_copy(l, rows, n).start()

    def finish_halo(l, rows, n):
        @pl.when(me_sp > 0)
        def _():
            halo_copy(l, rows, n).wait_recv()
            got = halo[l, rows, :]
            put_dup(got[:, :kv_width], got[:, kv_width:], rows)

    @pl.when(me_sp == 0)
    def _():
        none = jnp.zeros((row_count, 256), BF16)
        for kv in range(kv_heads):
            kdup[kv, 0:row_count, :] = none[:, :128]
            vdup[kv, 0:row_count, :] = none

    def attend_part(l, seg, kv, rows_at, lanes):
        rows = seg_rows(seg)
        stack = []
        for p in range(group // 2):
            lower = (kv * group + 2 * p) * HEAD_DIM
            tile = queries[rows, lower : lower + 128]
            none = jnp.zeros_like(tile)
            stack += [jnp.where(low_half, tile, none), jnp.where(low_half, none, tile)]
        stacked = jnp.concatenate(stack, axis=0)
        scores = lax.dot_general(
            stacked, kdup[kv, rows_at, :], (((1,), (1,)), ((), ())), preferred_element_type=F32
        )
        base = kv * group * SEG
        table = jnp.where(me_sp == 0, jnp.minimum(seg, 2), 2)
        expon = jnp.exp2(scores + bias[l, table, base : base + group * SEG, lanes]).astype(BF16)
        return jnp.dot(expon, vdup[kv, rows_at, :], preferred_element_type=F32)

    def put_mixed(seg, kv, summed):
        rows = seg_rows(seg)
        for p in range(group // 2):
            lower = (kv * group + 2 * p) * HEAD_DIM
            even = summed[2 * p * SEG : (2 * p + 1) * SEG]
            odd = summed[(2 * p + 1) * SEG : (2 * p + 2) * SEG]
            top = jnp.where(low_half, even[:, :128], odd[:, :128])
            under = jnp.where(low_half, even[:, 128:], odd[:, 128:])
            mixed[rows, lower : lower + 128] = (top / under).astype(BF16)

    def attend(l, seg):
        window = pl.ds(pl.multiple_of(seg * SEG, SEG), SPAN)
        for kv in range(kv_heads):
            put_mixed(seg, kv, attend_part(l, seg, kv, window, slice(0, SPAN)))

    late_keys = pl.ds(last * SEG, 2 * SEG)
    early_keys = pl.ds((last + 2) * SEG, SPAN - 2 * SEG)

    def attend_ahead(l):
        for kv in range(kv_heads):
            ahead[kv] = attend_part(l, last, kv, early_keys, slice(2 * SEG, SPAN))

    def attend_rest(l):
        for kv in range(kv_heads):
            rest = attend_part(l, last, kv, late_keys, slice(0, 2 * SEG))
            put_mixed(last, kv, ahead[kv] + rest)

    def project_out(l, rows, lower, size):
        cols = pl.ds(pl.multiple_of(lower, 128), size)
        return jnp.dot(mixed[rows, :], wo[l, :, cols], preferred_element_type=F32)

    def meet():
        at_edge = jnp.logical_or(me_sp == 0, me_sp == n_sp - 1)

        @pl.when(at_edge)
        def _():
            pl.semaphore_wait(barrier, n_x + min(n_sp - 1, 1))

        @pl.when(jnp.logical_not(at_edge))
        def _():
            pl.semaphore_wait(barrier, n_x + 2)

    early_load.wait()
    attn_gain_load.wait()
    take_rows(0, cur0, early)
    wk_load.wait()
    wv_load.wait()
    key_gain_load.wait()
    keys, values = keys_values(0, early)
    pair_made[0, early, :] = jnp.concatenate([keys, values], axis=1)
    meet()
    start_halo(0, early, last, core == 0)
    put_dup(keys, values, pl.ds(row_count + last * SEG, SEG))
    late_load.wait()
    take_rows(0, cur0, late)
    start_halo(0, early, last, core == 1)
    rel_bias_load.wait()
    build_line()
    keys, values = keys_values(0, late)
    pair_made[0, late, :] = jnp.concatenate([keys, values], axis=1)
    start_halo(0, late, 0)
    put_dup(keys, values, pl.ds(row_count, last * SEG))
    query_gain_load.wait()
    wq_load.wait()
    make_queries(0, early)
    build_bias(0)
    out_step = min(half_width, 512)
    whole_piece = pl.ds(0, half_width)
    first_pieces = [pl.ds(lower, out_step) for lower in range(0, half_width, out_step)]

    def pieces_of(i):
        if isinstance(i, int) and i == 0:
            return [(0 if n == 0 else segs + n - 1, cols) for n, cols in enumerate(first_pieces)]
        return [(i, whole_piece)]

    def partner_copy(i, n, cols):
        return send(
            psend.at[i, :, cols], precv.at[i, :, cols], ps_sem.at[0], pr_sem.at[n], partner
        )

    def chip_copy(i, k, n, cols):
        return send(
            xsend.at[i, :, cols],
            xrecv.at[k - 1, i, :, cols],
            xs_sem.at[k - 1],
            xr_sem.at[k - 1, n],
            peer(k),
        )

    my_half = pl.ds(pl.multiple_of(my_part * half_width, 128), half_width)

    def rows_copy(i, seg):
        rows = seg_rows(seg)
        return send(
            cur1.at[rows, my_half], cur1.at[rows, my_half], cs_sem.at[0], cr_sem.at[i], partner
        )

    def first_partner(i):
        for n, cols in pieces_of(i):
            for lower in range(cols.start, cols.start + cols.size, out_step):
                psend[i, :, lower : lower + out_step] = project_out(
                    0, seg_rows(last - i), (1 - my_part) * half_width + lower, out_step
                ).astype(BF16)
            partner_copy(i, n, cols).start()

    def first_own(i):
        for lower in range(0, half_width, out_step):
            own0[i, :, lower : lower + out_step] = project_out(
                0, seg_rows(last - i), my_part * half_width + lower, out_step
            )

    def first_sends(i):
        for n, cols in pieces_of(i):
            partner_copy(i, n, cols).wait_recv()
            both = own0[i, :, cols] + precv[i, :, cols].astype(F32)
            own0[i, :, cols] = both
            xsend[i, :, cols] = both.astype(BF16)
            for k in range(1, n_x):
                chip_copy(i, k, n, cols).start()

    attend_ahead(0)
    finish_halo(0, early, last)
    wo_load.wait()
    attend_rest(0)
    first_partner(0)
    first_own(0)
    first_sends(0)
    make_queries(0, seg_rows(last - 1))
    second_loads = [
        load(2, w_key.at[1], kv_part(1, 0)),
        load(3, w_value.at[1], kv_part(1, 1)),
        load(8, w_query.at[1], wq.at[1]),
        load(9, w_out.at[1], wo.at[1]),
    ]
    finish_halo(0, late, 0)
    attend(0, last - 1)
    first_partner(1)
    first_own(1)
    make_queries(0, pl.ds(0, (last - 1) * SEG))
    build_edge(0)
    first_sends(1)

    def first_round(i, carry):
        attend(0, last - i)
        first_partner(i)

        @pl.when(i > 2)
        def _():
            first_sends(i - 1)

        first_own(i)
        return carry

    lax.fori_loop(2, segs, first_round, 0)
    first_sends(last)

    def gather_rows(i, seg):
        rows = seg_rows(seg)
        total = own0[i]
        for k in range(1, n_x):
            for n, cols in pieces_of(i):
                chip_copy(i, k, n, cols).wait_recv()
            total = total + xrecv[k - 1, i].astype(F32)
        mine = (cur0[rows, my_half].astype(F32) + total).astype(BF16)
        cur1[rows, my_half] = mine
        rows_copy(i, seg).start()
        return half_rows(seg, my_half)

    def half_rows(seg, half):
        rows = seg_rows(seg)
        x = cur1[rows, half].astype(F32)
        gained[rows, half] = (x * attn_gain[1:2, half]).astype(BF16)
        return row_squares(x), half_dot(1, rows, half)

    their_half = pl.ds(pl.multiple_of((1 - my_part) * half_width, 128), half_width)

    def second_keys(i, seg, squares, flat):
        rows = seg_rows(seg)
        rows_copy(i, seg).wait_recv()
        more_squares, more_flat = half_rows(seg, their_half)
        scales[rows, :] = row_scale(squares + more_squares, width)
        keys, values = split_keys(1, rows, flat + more_flat)
        pair_made[1, rows, :] = jnp.concatenate([keys, values], axis=1)
        start_halo(1, rows, segs + seg)
        put_dup(keys, values, pl.ds(pl.multiple_of(row_count + seg * SEG, SEG), SEG))

    for copy in second_loads:
        copy.wait()
    begun = gather_rows(0, last)
    build_bias(1)
    build_edge(1)
    second_keys(0, last, *begun)

    def second_round(i, carry):
        begun = gather_rows(i, last - i)
        make_queries(1, seg_rows(segs - i))
        second_keys(i, last - i, *begun)
        return carry

    lax.fori_loop(1, last, second_round, 0)
    begun = gather_rows(last, 0)
    make_queries(1, seg_rows(1))
    attend_ahead(1)
    finish_halo(1, seg_rows(last), segs + last)
    second_keys(last, 0, *begun)

    groups = tuple(pl.ds(seg * SEG, SEG) for seg in reversed(range(segs)))

    def partner_copy1(g, k):
        rows = groups[g]
        return send(
            psend1.at[k, rows], precv1.at[k, rows], ps1_sem.at[0], pr_sem.at[g * n_x + k], partner
        )

    def chip_copy1(g, k):
        rows = groups[g]
        return send(
            xsend1.at[k - 1, rows],
            xrecv1.at[k - 1, rows],
            xs1_sem.at[k - 1],
            xr1_sem.at[k - 1, g],
            peer(k),
        )

    far = range(1, n_x)

    def last_partner(g, which):
        for k in which:
            lower = (chip_at(k) * 2 + 1 - core_at(k)) * feat
            psend1[k, groups[g], :] = project_out(1, groups[g], lower, feat).astype(BF16)
            partner_copy1(g, k).start()

    def last_own(g, which):
        for k in which:
            lower = (chip_at(k) * 2 + core_at(k)) * feat
            own1[k, groups[g], :] = project_out(1, groups[g], lower, feat)

    def last_sends(g):
        for k in far:
            partner_copy1(g, k).wait_recv()
            both = own1[k, groups[g], :] + precv1[k, groups[g], :].astype(F32)
            xsend1[k - 1, groups[g], :] = both.astype(BF16)
            chip_copy1(g, k).start()

    attend_rest(1)
    last_partner(0, far)
    for g in range(1, segs):
        if g == last:
            make_queries(1, seg_rows(0))
            last_own(g - 1, far)
            last_sends(g - 1)
        finish_halo(1, seg_rows(last - g), segs + last - g)
        attend(1, last - g)
        if g < last:
            last_own(g - 1, far)
            last_partner(g - 1, [0])
            last_sends(g - 1)
        last_partner(g, far)
    last_partner(last - 1, [0])
    last_own(last, far)
    last_partner(last, [0])
    last_own(0, [0])
    last_sends(last)
    for g in range(1, segs):
        last_own(g, [0])
    my_cols = pl.ds(pl.multiple_of(me_tp * feat, 128), feat)
    for g in range(len(groups)):
        rows = groups[g]
        partner_copy1(g, 0).wait_recv()
        total = cur1[rows, my_cols].astype(F32) + own1[0, rows, :] + precv1[0, rows, :].astype(F32)
        for k in range(1, n_x):
            chip_copy1(g, k).wait_recv()
            total = total + xrecv1[k - 1, rows, :].astype(F32)
        out[rows, :] = total.astype(BF16)

    send(psend, precv, ps_sem.at[0], pr_sem.at[0], partner).wait_send()
    send(cur1.at[:, my_half], cur1.at[:, my_half], cs_sem.at[0], cr_sem.at[0], partner).wait_send()
    send(psend1, precv1, ps1_sem.at[0], pr_sem.at[0], partner).wait_send()
    for k in range(1, n_x):
        send(xsend, xrecv.at[k - 1], xs_sem.at[k - 1], xr_sem.at[k - 1, 0], peer(k)).wait_send()
        send(
            xsend1.at[k - 1], xrecv1.at[k - 1], xs1_sem.at[k - 1], xr1_sem.at[k - 1, 0], peer(k)
        ).wait_send()

    @pl.when(me_sp < n_sp - 1)
    def _():
        for l in range(LAYERS):
            send(
                pair_made.at[l], halo.at[l], hs_sem.at[l], hr_sem.at[0],
                {"sp": lax.rem(me_sp + 1, n_sp)},
            ).wait_send()


def local(n_sp, n_tp, stream, attn_gain, w_query, w_key, w_value, w_out, query_gain, key_gain, rel_bias):
    row_count, width = stream.shape
    segs = row_count // SEG
    assert row_count == LEFT * SEG and n_tp % 2 == 0
    n_x = n_tp // 2
    feat = width // n_tp
    half_width = width // 2
    q_width = w_query.shape[2]
    kv_width = w_key.shape[2]
    kv_heads = kv_width // HEAD_DIM
    heads = q_width // HEAD_DIM
    group = heads // kv_heads
    others = max(n_x - 1, 1)
    dma = pltpu.SemaphoreType.DMA
    anyw = pl.BlockSpec(memory_space=pltpu.HBM)
    vmem = pl.BlockSpec(memory_space=pltpu.VMEM)
    scratch = [
        pltpu.VMEM(attn_gain.shape, F32),
        pltpu.VMEM(query_gain.shape, F32),
        pltpu.VMEM(key_gain.shape, F32),
        pltpu.VMEM(rel_bias.shape, F32),
        pltpu.VMEM((row_count, width), BF16),
        pltpu.VMEM((row_count, width), BF16),
        pltpu.VMEM((row_count, width), BF16),
        pltpu.VMEM((row_count, 128), F32),
        pltpu.VMEM(w_query.shape, BF16),
        pltpu.VMEM(
            (LAYERS, width, 2 * kv_width) if kv_width % 128 == 0 else (LAYERS, 2, width, kv_width),
            BF16,
        ),
        pltpu.VMEM(w_out.shape, BF16),
        pltpu.VMEM((row_count, q_width), BF16),
        pltpu.VMEM((LAYERS, row_count, 2 * kv_width), BF16),
        pltpu.VMEM((LAYERS, row_count, 2 * kv_width), BF16),
        pltpu.VMEM((kv_heads, 2 * row_count, 128), BF16),
        pltpu.VMEM((kv_heads, 2 * row_count, 256), BF16),
        pltpu.VMEM((LAYERS * heads, LINE), F32),
        pltpu.VMEM((LAYERS, 3, heads * SEG, LINE), F32),
        pltpu.VMEM((kv_heads, group * SEG, 256), F32),
        pltpu.VMEM((row_count, q_width), BF16),
        pltpu.VMEM((segs, SEG, half_width), BF16),
        pltpu.VMEM((segs, SEG, half_width), BF16),
        pltpu.VMEM((segs, SEG, half_width), F32),
        pltpu.VMEM((segs, SEG, half_width), BF16),
        pltpu.VMEM((others, segs, SEG, half_width), BF16),
        pltpu.VMEM((n_x, row_count, feat), BF16),
        pltpu.VMEM((n_x, row_count, feat), BF16),
        pltpu.VMEM((n_x, row_count, feat), F32),
        pltpu.VMEM((others, row_count, feat), BF16),
        pltpu.VMEM((others, row_count, feat), BF16),
        dma((10,)),
        dma((1,)), dma((max(segs * n_x, 2 * segs),)),
        dma((others,)), dma((others, segs + half_width // min(half_width, 512) - 1)),
        dma((1,)), dma((segs,)),
        dma((LAYERS,)), dma((LAYERS * segs,)),
        dma((1,)),
        dma((others,)), dma((others, segs)),
    ]
    return pl.pallas_call(
        functools.partial(body, n_sp, n_tp),
        out_shape=pltpu.VMEM((row_count, feat), BF16),
        in_specs=[anyw] * 9,
        out_specs=vmem,
        scratch_shapes=scratch,
        compiler_params=pltpu.CompilerParams(
            collective_id=0, has_side_effects=True, vmem_limit_bytes=60 * 1024 * 1024
        ),
    )(stream, attn_gain, w_query, w_key, w_value, w_out, query_gain, key_gain, rel_bias)


def solution(mesh):
    return jax.shard_map(
        functools.partial(local, mesh.shape["sp"], mesh.shape["tp"]),
        mesh=mesh,
        in_specs=(
            P("sp", None),
            P(),
            P(None, None, "tp"),
            P(None, None, "tp"),
            P(None, None, "tp"),
            P(None, "tp", None),
            P(),
            P(),
            P(None, "tp", None),
        ),
        out_specs=P("sp", "tp"),
        check_vma=False,
    )
```

```python
import functools

import jax
import jax.numpy as jnp
from jax import lax
from jax.experimental import pallas as pl
from jax.experimental.pallas import tpu as pltpu
from jax.sharding import PartitionSpec as P

HEAD_DIM = 64
SEG = 64
LEFT = 4
CLIP = 128
LAYERS = 2
SPAN = (LEFT + 1) * SEG
LINE = 384
LOG2E = 1.4426950408889634

norm_eps = 1e-06
masked_score = -1e30
F32 = jnp.float32
BF16 = jnp.bfloat16


def seg_rows(seg):
    return pl.ds(pl.multiple_of(seg * SEG, SEG), SEG)


def send(src, dst, send_sem, recv_sem, device):
    return pltpu.make_async_remote_copy(
        src_ref=src,
        dst_ref=dst,
        send_sem=send_sem,
        recv_sem=recv_sem,
        device_id=device,
        device_id_type=pl.DeviceIdType.MESH,
    )


def row_squares(x):
    return jnp.sum(x * x, axis=-1, keepdims=True)


def row_scale(squares, width):
    scale = lax.rsqrt(squares * (1.0 / width) + norm_eps)
    return jnp.broadcast_to(scale, (squares.shape[0], 128))


def widen(scale, width):
    return jnp.concatenate([scale] * -(-width // 128), axis=1)[:, :width]


def head_norm(x, gain_row, scale):
    width = x.shape[1]
    block = min(width, 256)
    row_head = lax.broadcasted_iota(jnp.int32, (block, block), 0) >> 6
    col_head = lax.broadcasted_iota(jnp.int32, (block, block), 1) >> 6
    spread = jnp.where(row_head == col_head, 1.0 / HEAD_DIM, 0.0).astype(BF16)
    gain = jnp.concatenate([gain_row] * (block // HEAD_DIM), axis=1) * scale
    outs = []
    for lower in range(0, width, block):
        part = x[:, lower : lower + block]
        mean = jnp.dot((part * part).astype(BF16), spread, preferred_element_type=F32)
        outs.append((part * lax.rsqrt(mean + norm_eps) * gain).astype(BF16))
    return outs[0] if len(outs) == 1 else jnp.concatenate(outs, axis=1)


def body(
    n_sp, n_tp,
    stream, attn_gain_in, w_query, w_key, w_value, w_out, query_gain_in, key_gain_in, rel_bias_in,
    out,
    attn_gain, query_gain, key_gain, rel_bias,
    cur0, cur1, gained, scales, wq, wkv, wo, queries, pair_made, halo, kdup, vdup, line, bias, ahead, mixed,
    psend, precv, own0, xsend, xrecv,
    psend1, precv1, own1, xsend1, xrecv1,
    w_sem, ps_sem, pr_sem, xs_sem, xr_sem, cr_sem, hs_sem, hr_sem, xr1_sem,
):
    row_count, width = cur0.shape
    segs = row_count // SEG
    q_width = wq.shape[2]
    kv_width = w_key.shape[2]
    heads = q_width // HEAD_DIM
    kv_heads = kv_width // HEAD_DIM
    group = heads // kv_heads
    n_x = n_tp // 2
    feat = width // n_tp
    half_width = width // 2
    last = segs - 1
    me_sp = lax.axis_index("sp")
    me_tp = lax.axis_index("tp")
    core = lax.rem(me_tp, 2)
    chip = lax.div(me_tp, 2)
    partner = {"tp": chip * 2 + 1 - core}

    def chip_at(k):
        return lax.rem(chip + k, n_x)

    def core_at(k):
        return lax.rem(core + k, 2)

    def peer(k):
        return {"tp": chip_at(k) * 2 + core_at(k)}

    my_part = lax.rem(core + chip, 2)

    barrier = pltpu.get_barrier_semaphore()
    pl.semaphore_signal(barrier, inc=1, device_id=partner, device_id_type=pl.DeviceIdType.MESH)
    for k in range(1, n_x):
        pl.semaphore_signal(barrier, inc=1, device_id=peer(k), device_id_type=pl.DeviceIdType.MESH)

    @pl.when(me_sp > 0)
    def _():
        pl.semaphore_signal(
            barrier, inc=1, device_id={"sp": me_sp - 1}, device_id_type=pl.DeviceIdType.MESH
        )

    @pl.when(me_sp < n_sp - 1)
    def _():
        pl.semaphore_signal(
            barrier, inc=1, device_id={"sp": me_sp + 1}, device_id_type=pl.DeviceIdType.MESH
        )

    def load(n, src, dst):
        copy = pltpu.make_async_copy(src, dst, w_sem.at[n])
        copy.start()
        return copy

    early = pl.ds(last * SEG, SEG)
    late = pl.ds(0, last * SEG)
    for lower in range(last * SEG, row_count, 16):
        load(0, stream.at[pl.ds(lower, 16)], cur0.at[pl.ds(lower, 16)])
    early_load = pltpu.make_async_copy(stream.at[early], cur0.at[early], w_sem.at[0])
    attn_gain_load = load(1, attn_gain_in, attn_gain)
    joined = kv_width % 128 == 0

    def kv_part(l, n):
        if joined:
            return wkv.at[l, :, pl.ds(n * kv_width, kv_width)]
        return wkv.at[l, n]

    wk_load = load(2, w_key.at[0], kv_part(0, 0))
    wv_load = load(3, w_value.at[0], kv_part(0, 1))
    key_gain_load = load(4, key_gain_in, key_gain)
    late_load = load(5, stream.at[late], cur0.at[late])
    rel_bias_load = load(6, rel_bias_in, rel_bias)
    query_gain_load = load(7, query_gain_in, query_gain)
    wq_load = load(8, w_query.at[0], wq.at[0])
    wo_load = load(9, w_out.at[0], wo.at[0])

    low_half = lax.broadcasted_iota(jnp.int32, (SEG, 128), 1) < HEAD_DIM

    def build_line():
        offset = lax.broadcasted_iota(jnp.int32, (2 * CLIP, LINE), 1)
        distance = jnp.clip(LEFT * SEG + SEG - 1 - offset, -CLIP, CLIP) + CLIP
        match = lax.broadcasted_iota(jnp.int32, (2 * CLIP, LINE), 0) == distance
        onehot = jnp.where(match, 1.0, 0.0).astype(BF16)
        far = (distance[:1] == 2 * CLIP).astype(F32)
        table = jnp.concatenate([rel_bias[l] for l in range(LAYERS)], axis=0)
        near = table[:, : 2 * CLIP]
        high = near.astype(BF16)
        near = near - high.astype(F32)
        middle = near.astype(BF16)
        low = (near - middle.astype(F32)).astype(BF16)
        high, middle, low = (
            jnp.dot(part, onehot, preferred_element_type=F32) for part in (high, middle, low)
        )
        line[...] = (high + middle + low + table[:, 2 * CLIP :] * far) * LOG2E

    def build_bias(l):
        for h in range(heads):
            row = slice(l * heads + h, l * heads + h + 1)
            spread = jnp.broadcast_to(line[row, 128:], (SEG, LINE - 128))
            turned = pltpu.roll(spread, LINE - 128 - (SEG - 1), 1, stride=1, stride_axis=0)
            tiles = [
                jnp.broadcast_to(line[row, :128], (SEG, 128)),
                turned[:, :128],
                jnp.where(low_half, turned[:, 128:], masked_score),
            ]
            top = jnp.maximum(jnp.maximum(tiles[0], tiles[1]), tiles[2])
            peak = jnp.max(top, axis=-1, keepdims=True)
            for n in range(3):
                bias[l, 2, h * SEG : (h + 1) * SEG, n * 128 : (n + 1) * 128] = tiles[n] - peak

    def build_edge(l):
        @pl.when(me_sp == 0)
        def _():
            for h in range(heads):
                rows = slice(h * SEG, (h + 1) * SEG)
                near = bias[l, 2, rows, 256:]
                middle = jnp.where(low_half, masked_score, bias[l, 2, rows, 128:256])
                shut = jnp.full((SEG, 128), masked_score, F32)
                peak = jnp.max(near, axis=-1, keepdims=True)
                bias[l, 0, rows, :128] = shut
                bias[l, 0, rows, 128:256] = shut
                bias[l, 0, rows, 256:] = near - peak
                peak = jnp.maximum(peak, jnp.max(middle, axis=-1, keepdims=True))
                bias[l, 1, rows, :128] = shut
                bias[l, 1, rows, 128:256] = middle - peak
                bias[l, 1, rows, 256:] = near - peak

    for kv in range(kv_heads):
        vdup[kv, :, 128:] = jnp.ones((2 * row_count, 128), BF16)

    def take_rows(l, current, rows):
        x = current[rows, :].astype(F32)
        gained[rows, :] = (x * attn_gain[l : l + 1]).astype(BF16)
        scales[rows, :] = row_scale(row_squares(x), width)

    halves = [pl.ds(n * half_width, half_width) for n in range(2)]

    def half_dot(l, rows, half):
        if joined:
            both = wkv[l, half, :]
        else:
            both = jnp.concatenate([wkv[l, 0, half, :], wkv[l, 1, half, :]], axis=1)
        return jnp.dot(gained[rows, half], both, preferred_element_type=F32)

    def keys_values(l, rows):
        row_scales = widen(scales[rows, :], 2 * kv_width)
        flat = half_dot(l, rows, halves[0]) * row_scales + half_dot(l, rows, halves[1]) * row_scales
        return split_keys(l, flat)

    def split_keys(l, flat):
        keys = head_norm(flat[:, :kv_width], key_gain[l : l + 1], 1.0)
        return keys, flat[:, kv_width:].astype(BF16)

    def make_queries(l, rows):
        flat = jnp.dot(gained[rows, :], wq[l], preferred_element_type=F32)
        queries[rows, :] = head_norm(
            flat * widen(scales[rows, :], q_width),
            query_gain[l : l + 1],
            HEAD_DIM ** (-0.5) * LOG2E,
        )

    def put_dup(keys, values, rows):
        for kv in range(kv_heads):
            cols = slice(kv * HEAD_DIM, (kv + 1) * HEAD_DIM)
            kdup[kv, rows, :] = jnp.concatenate([keys[:, cols]] * 2, axis=1)
            vdup[kv, rows, :128] = jnp.concatenate([values[:, cols]] * 2, axis=1)

    def halo_copy(l, rows, n):
        return send(
            pair_made.at[l, rows],
            halo.at[l, rows],
            hs_sem.at[0],
            hr_sem.at[n],
            {"sp": lax.rem(me_sp + 1, n_sp)},
        )

    def start_halo(l, rows, n, here=True):
        @pl.when(jnp.logical_and(me_sp < n_sp - 1, here))
        def _():
            halo_copy(l, rows, n).start()

    def end_halo(l):
        @pl.when(me_sp < n_sp - 1)
        def _():
            send(
                pair_made.at[l], halo.at[l], hs_sem.at[0], hr_sem.at[0],
                {"sp": lax.rem(me_sp + 1, n_sp)},
            ).wait_send()

    def finish_halo(l, rows, n):
        @pl.when(me_sp > 0)
        def _():
            halo_copy(l, rows, n).wait_recv()
            got = halo[l, rows, :]
            put_dup(got[:, :kv_width], got[:, kv_width:], rows)

    @pl.when(me_sp == 0)
    def _():
        none = jnp.zeros((row_count, 256), BF16)
        for kv in range(kv_heads):
            kdup[kv, 0:row_count, :] = none[:, :128]
            vdup[kv, 0:row_count, :] = none

    def attend_part(l, seg, kv, rows_at, lanes):
        rows = seg_rows(seg)
        stack = []
        for p in range(group // 2):
            lower = (kv * group + 2 * p) * HEAD_DIM
            tile = queries[rows, lower : lower + 128]
            none = jnp.zeros_like(tile)
            stack += [jnp.where(low_half, tile, none), jnp.where(low_half, none, tile)]
        stacked = jnp.concatenate(stack, axis=0)
        scores = lax.dot_general(
            stacked, kdup[kv, rows_at, :], (((1,), (1,)), ((), ())), preferred_element_type=F32
        )
        base = kv * group * SEG
        table = jnp.where(me_sp == 0, jnp.minimum(seg, 2), 2)
        expon = jnp.exp2(scores + bias[l, table, base : base + group * SEG, lanes]).astype(BF16)
        return jnp.dot(expon, vdup[kv, rows_at, :], preferred_element_type=F32)

    def put_mixed(seg, kv, summed):
        rows = seg_rows(seg)
        for p in range(group // 2):
            lower = (kv * group + 2 * p) * HEAD_DIM
            even = summed[2 * p * SEG : (2 * p + 1) * SEG]
            odd = summed[(2 * p + 1) * SEG : (2 * p + 2) * SEG]
            top = jnp.where(low_half, even[:, :128], odd[:, :128])
            under = jnp.where(low_half, even[:, 128:], odd[:, 128:])
            mixed[rows, lower : lower + 128] = (top / under).astype(BF16)

    def attend(l, seg):
        window = pl.ds(pl.multiple_of(seg * SEG, SEG), SPAN)
        for kv in range(kv_heads):
            put_mixed(seg, kv, attend_part(l, seg, kv, window, slice(0, SPAN)))

    late_keys = pl.ds(last * SEG, 2 * SEG)
    early_keys = pl.ds((last + 2) * SEG, SPAN - 2 * SEG)

    def attend_ahead(l):
        for kv in range(kv_heads):
            ahead[kv] = attend_part(l, last, kv, early_keys, slice(2 * SEG, SPAN))

    def attend_rest(l):
        for kv in range(kv_heads):
            rest = attend_part(l, last, kv, late_keys, slice(0, 2 * SEG))
            put_mixed(last, kv, ahead[kv] + rest)

    def project_out(l, rows, lower, size):
        cols = pl.ds(pl.multiple_of(lower, 128), size)
        return jnp.dot(mixed[rows, :], wo[l, :, cols], preferred_element_type=F32)

    def meet():
        at_edge = jnp.logical_or(me_sp == 0, me_sp == n_sp - 1)

        @pl.when(at_edge)
        def _():
            pl.semaphore_wait(barrier, n_x + min(n_sp - 1, 1))

        @pl.when(jnp.logical_not(at_edge))
        def _():
            pl.semaphore_wait(barrier, n_x + 2)

    early_load.wait()
    attn_gain_load.wait()
    take_rows(0, cur0, early)
    wk_load.wait()
    wv_load.wait()
    key_gain_load.wait()
    keys, values = keys_values(0, early)
    pair_made[0, early, :] = jnp.concatenate([keys, values], axis=1)
    meet()
    start_halo(0, early, 1, core == 0)
    put_dup(keys, values, pl.ds(row_count + last * SEG, SEG))
    late_load.wait()
    take_rows(0, cur0, late)
    start_halo(0, early, 1, core == 1)
    rel_bias_load.wait()
    build_line()
    keys, values = keys_values(0, late)
    pair_made[0, late, :] = jnp.concatenate([keys, values], axis=1)
    start_halo(0, late, 0)
    put_dup(keys, values, pl.ds(row_count, last * SEG))
    query_gain_load.wait()
    wq_load.wait()
    make_queries(0, early)
    build_bias(0)
    out_step = min(half_width, 512)
    whole_piece = pl.ds(0, half_width)
    first_pieces = [pl.ds(lower, out_step) for lower in range(0, half_width, out_step)]

    def pieces_of(i):
        if isinstance(i, int) and i == 0:
            return [(0 if n == 0 else segs + n - 1, cols) for n, cols in enumerate(first_pieces)]
        return [(i, whole_piece)]

    def partner_copy(i, n, cols):
        return send(
            psend.at[i, :, cols], precv.at[i, :, cols], ps_sem.at[0], pr_sem.at[n], partner
        )

    def chip_copy(i, k, n, cols):
        return send(
            xsend.at[i, :, cols],
            xrecv.at[k - 1, i, :, cols],
            xs_sem.at[k - 1],
            xr_sem.at[k - 1, n],
            peer(k),
        )

    my_half = pl.ds(pl.multiple_of(my_part * half_width, 128), half_width)

    def rows_copy(i, seg):
        rows = seg_rows(seg)
        return send(
            cur1.at[rows, my_half], cur1.at[rows, my_half], ps_sem.at[0], cr_sem.at[i], partner
        )

    def first_partner(i):
        for n, cols in pieces_of(i):
            for lower in range(cols.start, cols.start + cols.size, out_step):
                psend[i, :, lower : lower + out_step] = project_out(
                    0, seg_rows(last - i), (1 - my_part) * half_width + lower, out_step
                ).astype(BF16)
            partner_copy(i, n, cols).start()

    def first_own(i):
        for lower in range(0, half_width, out_step):
            own0[i, :, lower : lower + out_step] = project_out(
                0, seg_rows(last - i), my_part * half_width + lower, out_step
            )

    def first_sends(i):
        for n, cols in pieces_of(i):
            partner_copy(i, n, cols).wait_recv()
            both = own0[i, :, cols] + precv[i, :, cols].astype(F32)
            own0[i, :, cols] = both
            xsend[i, :, cols] = both.astype(BF16)
            for k in range(1, n_x):
                chip_copy(i, k, n, cols).start()

    attend_ahead(0)
    finish_halo(0, early, 1)
    wo_load.wait()
    attend_rest(0)
    first_partner(0)
    first_own(0)
    first_sends(0)
    make_queries(0, seg_rows(last - 1))
    second_loads = [
        load(2, w_key.at[1], kv_part(1, 0)),
        load(3, w_value.at[1], kv_part(1, 1)),
        load(8, w_query.at[1], wq.at[1]),
        load(9, w_out.at[1], wo.at[1]),
    ]
    finish_halo(0, late, 0)
    attend(0, last - 1)
    first_partner(1)
    first_own(1)
    make_queries(0, pl.ds(0, (last - 1) * SEG))
    build_edge(0)
    first_sends(1)

    def first_round(i, carry):
        attend(0, last - i)
        first_partner(i)

        @pl.when(i > 2)
        def _():
            first_sends(i - 1)

        first_own(i)
        return carry

    lax.fori_loop(2, segs, first_round, 0)
    first_sends(last)

    def gather_rows(i, seg):
        rows = seg_rows(seg)
        total = own0[i]
        for k in range(1, n_x):
            for n, cols in pieces_of(i):
                chip_copy(i, k, n, cols).wait_recv()
            total = total + xrecv[k - 1, i].astype(F32)
        mine = (cur0[rows, my_half].astype(F32) + total).astype(BF16)
        cur1[rows, my_half] = mine
        rows_copy(i, seg).start()
        squares = half_rows(seg, my_half)
        return squares, half_dot(1, rows, my_half)

    def half_rows(seg, half):
        rows = seg_rows(seg)
        x = cur1[rows, half].astype(F32)
        gained[rows, half] = (x * attn_gain[1:2, half]).astype(BF16)
        return row_squares(x)

    their_start = (1 - my_part) * half_width
    their_half = pl.ds(pl.multiple_of(their_start, 128), half_width)
    quarters = [
        pl.ds(pl.multiple_of(their_start + n * (half_width // 2), 128), half_width // 2)
        for n in range(2)
    ]

    def second_keys(i, seg, squares, flat):
        rows = seg_rows(seg)
        rows_copy(i, seg).wait_recv()
        row_scales = row_scale(squares + half_rows(seg, their_half), width)
        scales[rows, :] = row_scales
        row_scales = widen(row_scales, 2 * kv_width)
        flat = flat * row_scales
        for part in quarters:
            flat = flat + half_dot(1, rows, part) * row_scales
        keys, values = split_keys(1, flat)
        pair_made[1, rows, :] = jnp.concatenate([keys, values], axis=1)
        start_halo(1, rows, 2 + seg)
        put_dup(keys, values, pl.ds(pl.multiple_of(row_count + seg * SEG, SEG), SEG))

    send(psend, precv, ps_sem.at[0], pr_sem.at[0], partner).wait_send()
    for copy in second_loads:
        copy.wait()
    begun = gather_rows(0, last)
    build_bias(1)
    build_edge(1)
    end_halo(0)
    second_keys(0, last, *begun)

    def second_round(i, carry):
        begun = gather_rows(i, last - i)
        make_queries(1, seg_rows(segs - i))
        second_keys(i, last - i, *begun)
        return carry

    lax.fori_loop(1, last, second_round, 0)
    begun = gather_rows(last, 0)
    make_queries(1, seg_rows(1))
    attend_ahead(1)
    finish_halo(1, seg_rows(last), 2 + last)
    second_keys(last, 0, *begun)

    groups = tuple(pl.ds(seg * SEG, SEG) for seg in reversed(range(segs)))

    def near(g, k):
        return segs if k == 0 else (g if k == 1 else segs + 1 + (k - 2) * segs + g)

    def partner_copy1(g, k):
        rows = groups[g]
        return send(
            psend1.at[k, rows], precv1.at[k, rows], ps_sem.at[0], pr_sem.at[near(g, k)], partner
        )

    def chip_copy1(g, k):
        rows = groups[g]
        return send(
            xsend1.at[k - 1, rows],
            xrecv1.at[k - 1, rows],
            xs_sem.at[k - 1],
            xr1_sem.at[k - 1, g],
            peer(k),
        )

    far = range(1, n_x)

    def last_partner(g, which):
        for k in which:
            lower = (chip_at(k) * 2 + 1 - core_at(k)) * feat
            psend1[k, groups[g], :] = project_out(1, groups[g], lower, feat).astype(BF16)
            partner_copy1(g, k).start()

    def last_own(g, which):
        for k in which:
            lower = (chip_at(k) * 2 + core_at(k)) * feat
            own1[k, groups[g], :] = project_out(1, groups[g], lower, feat)

    def last_sends(g):
        for k in far:
            partner_copy1(g, k).wait_recv()
            both = own1[k, groups[g], :] + precv1[k, groups[g], :].astype(F32)
            xsend1[k - 1, groups[g], :] = both.astype(BF16)
            chip_copy1(g, k).start()

    rows_sent = cur1.at[:, my_half]
    send(rows_sent, rows_sent, ps_sem.at[0], cr_sem.at[0], partner).wait_send()
    for k in far:
        send(xsend, xrecv.at[k - 1], xs_sem.at[k - 1], xr_sem.at[k - 1, 0], peer(k)).wait_send()
    attend_rest(1)
    last_partner(0, far)
    for g in range(1, segs):
        if g == last:
            make_queries(1, seg_rows(0))
            last_own(g - 1, far)
            last_sends(g - 1)
        finish_halo(1, seg_rows(last - g), 2 + last - g)
        attend(1, last - g)
        if g < last:
            last_own(g - 1, far)
            last_partner(g - 1, [0])
            last_sends(g - 1)
        last_partner(g, far)
    last_partner(last - 1, [0])
    last_own(last, far)
    last_partner(last, [0])
    last_own(0, [0])
    last_sends(last)
    for g in range(1, segs):
        last_own(g, [0])
    my_cols = pl.ds(pl.multiple_of(me_tp * feat, 128), feat)
    send(psend1.at[0], precv1.at[0], ps_sem.at[0], pr_sem.at[segs], partner).wait_recv()
    for g in range(len(groups)):
        rows = groups[g]
        total = cur1[rows, my_cols].astype(F32) + own1[0, rows, :] + precv1[0, rows, :].astype(F32)
        for k in range(1, n_x):
            chip_copy1(g, k).wait_recv()
            total = total + xrecv1[k - 1, rows, :].astype(F32)
        out[rows, :] = total.astype(BF16)

    send(psend1, precv1, ps_sem.at[0], pr_sem.at[0], partner).wait_send()
    for k in range(1, n_x):
        send(
            xsend1.at[k - 1], xrecv1.at[k - 1], xs_sem.at[k - 1], xr1_sem.at[k - 1, 0], peer(k)
        ).wait_send()
    end_halo(1)


def local(n_sp, n_tp, stream, attn_gain, w_query, w_key, w_value, w_out, query_gain, key_gain, rel_bias):
    row_count, width = stream.shape
    segs = row_count // SEG
    assert row_count == LEFT * SEG and n_tp % 2 == 0
    n_x = n_tp // 2
    feat = width // n_tp
    half_width = width // 2
    q_width = w_query.shape[2]
    kv_width = w_key.shape[2]
    kv_heads = kv_width // HEAD_DIM
    heads = q_width // HEAD_DIM
    group = heads // kv_heads
    others = max(n_x - 1, 1)
    dma = pltpu.SemaphoreType.DMA
    anyw = pl.BlockSpec(memory_space=pltpu.HBM)
    vmem = pl.BlockSpec(memory_space=pltpu.VMEM)
    scratch = [
        pltpu.VMEM(attn_gain.shape, F32),
        pltpu.VMEM(query_gain.shape, F32),
        pltpu.VMEM(key_gain.shape, F32),
        pltpu.VMEM(rel_bias.shape, F32),
        pltpu.VMEM((row_count, width), BF16),
        pltpu.VMEM((row_count, width), BF16),
        pltpu.VMEM((row_count, width), BF16),
        pltpu.VMEM((row_count, 128), F32),
        pltpu.VMEM(w_query.shape, BF16),
        pltpu.VMEM(
            (LAYERS, width, 2 * kv_width) if kv_width % 128 == 0 else (LAYERS, 2, width, kv_width),
            BF16,
        ),
        pltpu.VMEM(w_out.shape, BF16),
        pltpu.VMEM((row_count, q_width), BF16),
        pltpu.VMEM((LAYERS, row_count, 2 * kv_width), BF16),
        pltpu.VMEM((LAYERS, row_count, 2 * kv_width), BF16),
        pltpu.VMEM((kv_heads, 2 * row_count, 128), BF16),
        pltpu.VMEM((kv_heads, 2 * row_count, 256), BF16),
        pltpu.VMEM((LAYERS * heads, LINE), F32),
        pltpu.VMEM((LAYERS, 3, heads * SEG, LINE), F32),
        pltpu.VMEM((kv_heads, group * SEG, 256), F32),
        pltpu.VMEM((row_count, q_width), BF16),
        pltpu.VMEM((segs, SEG, half_width), BF16),
        pltpu.VMEM((segs, SEG, half_width), BF16),
        pltpu.VMEM((segs, SEG, half_width), F32),
        pltpu.VMEM((segs, SEG, half_width), BF16),
        pltpu.VMEM((others, segs, SEG, half_width), BF16),
        pltpu.VMEM((n_x, row_count, feat), BF16),
        pltpu.VMEM((n_x, row_count, feat), BF16),
        pltpu.VMEM((n_x, row_count, feat), F32),
        pltpu.VMEM((others, row_count, feat), BF16),
        pltpu.VMEM((others, row_count, feat), BF16),
        dma((10,)),
        dma((1,)), dma((segs + 1 + (others - 1) * segs,)),
        dma((others,)), dma((others, segs + half_width // min(half_width, 512) - 1)),
        dma((segs,)),
        dma((1,)), dma((2 + segs,)),
        dma((others, segs)),
    ]
    return pl.pallas_call(
        functools.partial(body, n_sp, n_tp),
        out_shape=pltpu.VMEM((row_count, feat), BF16),
        in_specs=[anyw] * 9,
        out_specs=vmem,
        scratch_shapes=scratch,
        compiler_params=pltpu.CompilerParams(
            collective_id=0, has_side_effects=True, vmem_limit_bytes=60 * 1024 * 1024
        ),
    )(stream, attn_gain, w_query, w_key, w_value, w_out, query_gain, key_gain, rel_bias)


def solution(mesh):
    return jax.shard_map(
        functools.partial(local, mesh.shape["sp"], mesh.shape["tp"]),
        mesh=mesh,
        in_specs=(
            P("sp", None),
            P(),
            P(None, None, "tp"),
            P(None, None, "tp"),
            P(None, None, "tp"),
            P(None, "tp", None),
            P(),
            P(),
            P(None, "tp", None),
        ),
        out_specs=P("sp", "tp"),
        check_vma=False,
    )
```

```python
import functools

import jax
import jax.numpy as jnp
from jax import lax
from jax.experimental import pallas as pl
from jax.experimental.pallas import tpu as pltpu
from jax.sharding import PartitionSpec as P

HEAD_DIM = 64
SEG = 64
LEFT = 4
CLIP = 128
LAYERS = 2
SPAN = (LEFT + 1) * SEG
LINE = 384
LOG2E = 1.4426950408889634
DIRECT = 16

norm_eps = 1e-06
masked_score = -1e30
F32 = jnp.float32
BF16 = jnp.bfloat16


def seg_rows(seg):
    return pl.ds(pl.multiple_of(seg * SEG, SEG), SEG)


def send(src, dst, send_sem, recv_sem, device):
    return pltpu.make_async_remote_copy(
        src_ref=src,
        dst_ref=dst,
        send_sem=send_sem,
        recv_sem=recv_sem,
        device_id=device,
        device_id_type=pl.DeviceIdType.MESH,
    )


def row_squares(x):
    return jnp.sum(x * x, axis=-1, keepdims=True)


def row_scale(squares, width):
    scale = lax.rsqrt(squares * (1.0 / width) + norm_eps)
    return jnp.broadcast_to(scale, (squares.shape[0], 128))


def widen(scale, width):
    return jnp.concatenate([scale] * -(-width // 128), axis=1)[:, :width]


def head_norm(x, gain_row, scale):
    width = x.shape[1]
    block = min(width, 256)
    row_head = lax.broadcasted_iota(jnp.int32, (block, block), 0) >> 6
    col_head = lax.broadcasted_iota(jnp.int32, (block, block), 1) >> 6
    spread = jnp.where(row_head == col_head, 1.0 / HEAD_DIM, 0.0).astype(BF16)
    gain = jnp.concatenate([gain_row] * (block // HEAD_DIM), axis=1) * scale
    outs = []
    for lower in range(0, width, block):
        part = x[:, lower : lower + block]
        mean = jnp.dot((part * part).astype(BF16), spread, preferred_element_type=F32)
        outs.append((part * lax.rsqrt(mean + norm_eps) * gain).astype(BF16))
    return outs[0] if len(outs) == 1 else jnp.concatenate(outs, axis=1)


def body(
    n_sp, n_tp,
    stream, attn_gain_in, w_query, w_key, w_value, w_out, query_gain_in, key_gain_in, rel_bias_in,
    out,
    attn_gain, query_gain, key_gain, rel_bias,
    cur0, cur1, gained, scales, wq, wkv, wo, queries, pair_made, halo, kdup, vdup, line, bias, ahead, mixed,
    psend, precv, own0, xsend, xrecv,
    psend1, precv1, own1, xsend1, xrecv1, dsend, drecv,
    w_sem, ps_sem, pr_sem, xs_sem, xr_sem, cr_sem, hs_sem, hr_sem, xr1_sem, ds_sem, dr_sem,
):
    row_count, width = cur0.shape
    segs = row_count // SEG
    q_width = wq.shape[2]
    kv_width = w_key.shape[2]
    heads = q_width // HEAD_DIM
    kv_heads = kv_width // HEAD_DIM
    group = heads // kv_heads
    n_x = n_tp // 2
    feat = width // n_tp
    half_width = width // 2
    last = segs - 1
    me_sp = lax.axis_index("sp")
    me_tp = lax.axis_index("tp")
    core = lax.rem(me_tp, 2)
    chip = lax.div(me_tp, 2)
    partner = {"tp": chip * 2 + 1 - core}

    def chip_at(k):
        return lax.rem(chip + k, n_x)

    def core_at(k):
        return lax.rem(core + k, 2)

    def peer(k):
        return {"tp": chip_at(k) * 2 + core_at(k)}

    def far_peer(k):
        return {"tp": chip_at(k) * 2 + 1 - core_at(k)}

    my_part = lax.rem(core + chip, 2)

    barrier = pltpu.get_barrier_semaphore()
    pl.semaphore_signal(barrier, inc=1, device_id=partner, device_id_type=pl.DeviceIdType.MESH)
    for k in range(1, n_x):
        for there in (peer(k), far_peer(k)):
            pl.semaphore_signal(barrier, inc=1, device_id=there, device_id_type=pl.DeviceIdType.MESH)

    @pl.when(me_sp > 0)
    def _():
        pl.semaphore_signal(
            barrier, inc=1, device_id={"sp": me_sp - 1}, device_id_type=pl.DeviceIdType.MESH
        )

    @pl.when(me_sp < n_sp - 1)
    def _():
        pl.semaphore_signal(
            barrier, inc=1, device_id={"sp": me_sp + 1}, device_id_type=pl.DeviceIdType.MESH
        )

    def load(n, src, dst):
        copy = pltpu.make_async_copy(src, dst, w_sem.at[n])
        copy.start()
        return copy

    early = pl.ds(last * SEG, SEG)
    late = pl.ds(0, last * SEG)
    for lower in range(last * SEG, row_count, 16):
        load(0, stream.at[pl.ds(lower, 16)], cur0.at[pl.ds(lower, 16)])
    early_load = pltpu.make_async_copy(stream.at[early], cur0.at[early], w_sem.at[0])
    attn_gain_load = load(1, attn_gain_in, attn_gain)
    joined = kv_width % 128 == 0

    def kv_part(l, n):
        if joined:
            return wkv.at[l, :, pl.ds(n * kv_width, kv_width)]
        return wkv.at[l, n]

    wk_load = load(2, w_key.at[0], kv_part(0, 0))
    wv_load = load(3, w_value.at[0], kv_part(0, 1))
    key_gain_load = load(4, key_gain_in, key_gain)
    late_load = load(5, stream.at[late], cur0.at[late])
    rel_bias_load = load(6, rel_bias_in, rel_bias)
    query_gain_load = load(7, query_gain_in, query_gain)
    wq_load = load(8, w_query.at[0], wq.at[0])
    wo_load = load(9, w_out.at[0], wo.at[0])

    low_half = lax.broadcasted_iota(jnp.int32, (SEG, 128), 1) < HEAD_DIM

    def build_line():
        offset = lax.broadcasted_iota(jnp.int32, (2 * CLIP, LINE), 1)
        distance = jnp.clip(LEFT * SEG + SEG - 1 - offset, -CLIP, CLIP) + CLIP
        match = lax.broadcasted_iota(jnp.int32, (2 * CLIP, LINE), 0) == distance
        onehot = jnp.where(match, 1.0, 0.0).astype(BF16)
        far = (distance[:1] == 2 * CLIP).astype(F32)
        table = jnp.concatenate([rel_bias[l] for l in range(LAYERS)], axis=0)
        near = table[:, : 2 * CLIP]
        high = near.astype(BF16)
        near = near - high.astype(F32)
        middle = near.astype(BF16)
        low = (near - middle.astype(F32)).astype(BF16)
        high, middle, low = (
            jnp.dot(part, onehot, preferred_element_type=F32) for part in (high, middle, low)
        )
        line[...] = (high + middle + low + table[:, 2 * CLIP :] * far) * LOG2E

    def build_bias(l):
        for h in range(heads):
            row = slice(l * heads + h, l * heads + h + 1)
            spread = jnp.broadcast_to(line[row, 128:], (SEG, LINE - 128))
            turned = pltpu.roll(spread, LINE - 128 - (SEG - 1), 1, stride=1, stride_axis=0)
            tiles = [
                jnp.broadcast_to(line[row, :128], (SEG, 128)),
                turned[:, :128],
                jnp.where(low_half, turned[:, 128:], masked_score),
            ]
            top = jnp.maximum(jnp.maximum(tiles[0], tiles[1]), tiles[2])
            peak = jnp.max(top, axis=-1, keepdims=True)
            for n in range(3):
                bias[l, 2, h * SEG : (h + 1) * SEG, n * 128 : (n + 1) * 128] = tiles[n] - peak

    def build_edge(l):
        @pl.when(me_sp == 0)
        def _():
            for h in range(heads):
                rows = slice(h * SEG, (h + 1) * SEG)
                near = bias[l, 2, rows, 256:]
                middle = jnp.where(low_half, masked_score, bias[l, 2, rows, 128:256])
                shut = jnp.full((SEG, 128), masked_score, F32)
                peak = jnp.max(near, axis=-1, keepdims=True)
                bias[l, 0, rows, :128] = shut
                bias[l, 0, rows, 128:256] = shut
                bias[l, 0, rows, 256:] = near - peak
                peak = jnp.maximum(peak, jnp.max(middle, axis=-1, keepdims=True))
                bias[l, 1, rows, :128] = shut
                bias[l, 1, rows, 128:256] = middle - peak
                bias[l, 1, rows, 256:] = near - peak

    for kv in range(kv_heads):
        vdup[kv, :, 128:] = jnp.ones((2 * row_count, 128), BF16)

    def take_rows(l, current, rows):
        x = current[rows, :].astype(F32)
        gained[rows, :] = (x * attn_gain[l : l + 1]).astype(BF16)
        scales[rows, :] = row_scale(row_squares(x), width)

    halves = [pl.ds(n * half_width, half_width) for n in range(2)]

    def half_dot(l, rows, half):
        if joined:
            both = wkv[l, half, :]
        else:
            both = jnp.concatenate([wkv[l, 0, half, :], wkv[l, 1, half, :]], axis=1)
        return jnp.dot(gained[rows, half], both, preferred_element_type=F32)

    def keys_values(l, rows):
        row_scales = widen(scales[rows, :], 2 * kv_width)
        flat = half_dot(l, rows, halves[0]) * row_scales + half_dot(l, rows, halves[1]) * row_scales
        return split_keys(l, flat)

    def split_keys(l, flat):
        keys = head_norm(flat[:, :kv_width], key_gain[l : l + 1], 1.0)
        return keys, flat[:, kv_width:].astype(BF16)

    def make_queries(l, rows):
        flat = jnp.dot(gained[rows, :], wq[l], preferred_element_type=F32)
        queries[rows, :] = head_norm(
            flat * widen(scales[rows, :], q_width),
            query_gain[l : l + 1],
            HEAD_DIM ** (-0.5) * LOG2E,
        )

    def put_dup(keys, values, rows):
        for kv in range(kv_heads):
            cols = slice(kv * HEAD_DIM, (kv + 1) * HEAD_DIM)
            kdup[kv, rows, :] = jnp.concatenate([keys[:, cols]] * 2, axis=1)
            vdup[kv, rows, :128] = jnp.concatenate([values[:, cols]] * 2, axis=1)

    def halo_copy(l, rows, n):
        return send(
            pair_made.at[l, rows],
            halo.at[l, rows],
            hs_sem.at[0],
            hr_sem.at[n],
            {"sp": lax.rem(me_sp + 1, n_sp)},
        )

    def start_halo(l, rows, n, here=True):
        @pl.when(jnp.logical_and(me_sp < n_sp - 1, here))
        def _():
            halo_copy(l, rows, n).start()

    def end_halo(l):
        @pl.when(me_sp < n_sp - 1)
        def _():
            send(
                pair_made.at[l], halo.at[l], hs_sem.at[0], hr_sem.at[0],
                {"sp": lax.rem(me_sp + 1, n_sp)},
            ).wait_send()

    def finish_halo(l, rows, n):
        @pl.when(me_sp > 0)
        def _():
            halo_copy(l, rows, n).wait_recv()
            got = halo[l, rows, :]
            put_dup(got[:, :kv_width], got[:, kv_width:], rows)

    @pl.when(me_sp == 0)
    def _():
        none = jnp.zeros((row_count, 256), BF16)
        for kv in range(kv_heads):
            kdup[kv, 0:row_count, :] = none[:, :128]
            vdup[kv, 0:row_count, :] = none

    def attend_part(l, seg, kv, rows_at, lanes):
        rows = seg_rows(seg)
        stack = []
        for p in range(group // 2):
            lower = (kv * group + 2 * p) * HEAD_DIM
            tile = queries[rows, lower : lower + 128]
            none = jnp.zeros_like(tile)
            stack += [jnp.where(low_half, tile, none), jnp.where(low_half, none, tile)]
        stacked = jnp.concatenate(stack, axis=0)
        scores = lax.dot_general(
            stacked, kdup[kv, rows_at, :], (((1,), (1,)), ((), ())), preferred_element_type=F32
        )
        base = kv * group * SEG
        table = jnp.where(me_sp == 0, jnp.minimum(seg, 2), 2)
        expon = jnp.exp2(scores + bias[l, table, base : base + group * SEG, lanes]).astype(BF16)
        return jnp.dot(expon, vdup[kv, rows_at, :], preferred_element_type=F32)

    def put_mixed(seg, kv, summed):
        rows = seg_rows(seg)
        for p in range(group // 2):
            lower = (kv * group + 2 * p) * HEAD_DIM
            even = summed[2 * p * SEG : (2 * p + 1) * SEG]
            odd = summed[(2 * p + 1) * SEG : (2 * p + 2) * SEG]
            top = jnp.where(low_half, even[:, :128], odd[:, :128])
            under = jnp.where(low_half, even[:, 128:], odd[:, 128:])
            mixed[rows, lower : lower + 128] = (top / under).astype(BF16)

    def attend(l, seg):
        window = pl.ds(pl.multiple_of(seg * SEG, SEG), SPAN)
        for kv in range(kv_heads):
            put_mixed(seg, kv, attend_part(l, seg, kv, window, slice(0, SPAN)))

    late_keys = pl.ds(last * SEG, 2 * SEG)
    early_keys = pl.ds((last + 2) * SEG, SPAN - 2 * SEG)

    def attend_ahead(l):
        for kv in range(kv_heads):
            ahead[kv] = attend_part(l, last, kv, early_keys, slice(2 * SEG, SPAN))

    def attend_rest(l):
        for kv in range(kv_heads):
            rest = attend_part(l, last, kv, late_keys, slice(0, 2 * SEG))
            put_mixed(last, kv, ahead[kv] + rest)

    def project_out(l, rows, lower, size):
        cols = pl.ds(pl.multiple_of(lower, 128), size)
        return jnp.dot(mixed[rows, :], wo[l, :, cols], preferred_element_type=F32)

    def meet():
        at_edge = jnp.logical_or(me_sp == 0, me_sp == n_sp - 1)

        @pl.when(at_edge)
        def _():
            pl.semaphore_wait(barrier, 2 * n_x - 1 + min(n_sp - 1, 1))

        @pl.when(jnp.logical_not(at_edge))
        def _():
            pl.semaphore_wait(barrier, 2 * n_x - 1 + 2)

    early_load.wait()
    attn_gain_load.wait()
    take_rows(0, cur0, early)
    wk_load.wait()
    wv_load.wait()
    key_gain_load.wait()
    keys, values = keys_values(0, early)
    pair_made[0, early, :] = jnp.concatenate([keys, values], axis=1)
    meet()
    start_halo(0, early, 1, core == 0)
    put_dup(keys, values, pl.ds(row_count + last * SEG, SEG))
    late_load.wait()
    take_rows(0, cur0, late)
    start_halo(0, early, 1, core == 1)
    rel_bias_load.wait()
    build_line()
    keys, values = keys_values(0, late)
    pair_made[0, late, :] = jnp.concatenate([keys, values], axis=1)
    start_halo(0, late, 0)
    put_dup(keys, values, pl.ds(row_count, last * SEG))
    query_gain_load.wait()
    wq_load.wait()
    make_queries(0, early)
    build_bias(0)
    out_step = min(half_width, 512)
    whole_piece = pl.ds(0, half_width)
    first_pieces = [pl.ds(lower, out_step) for lower in range(0, half_width, out_step)]

    def pieces_of(i):
        if isinstance(i, int) and i == 0:
            return [(0 if n == 0 else segs + n - 1, cols) for n, cols in enumerate(first_pieces)]
        return [(i, whole_piece)]

    def partner_copy(i, n, cols):
        return send(
            psend.at[i, :, cols], precv.at[i, :, cols], ps_sem.at[0], pr_sem.at[n], partner
        )

    def chip_copy(i, k, n, cols):
        return send(
            xsend.at[i, :, cols],
            xrecv.at[k - 1, i, :, cols],
            xs_sem.at[k - 1],
            xr_sem.at[k - 1, n],
            peer(k),
        )

    my_half = pl.ds(pl.multiple_of(my_part * half_width, 128), half_width)

    def rows_copy(i, seg):
        rows = seg_rows(seg)
        return send(
            cur1.at[rows, my_half], cur1.at[rows, my_half], ps_sem.at[0], cr_sem.at[i], partner
        )

    def first_partner(i):
        for n, cols in pieces_of(i):
            for lower in range(cols.start, cols.start + cols.size, out_step):
                psend[i, :, lower : lower + out_step] = project_out(
                    0, seg_rows(last - i), (1 - my_part) * half_width + lower, out_step
                ).astype(BF16)
            partner_copy(i, n, cols).start()

    def first_own(i):
        for lower in range(0, half_width, out_step):
            own0[i, :, lower : lower + out_step] = project_out(
                0, seg_rows(last - i), my_part * half_width + lower, out_step
            )

    def first_sends(i):
        for n, cols in pieces_of(i):
            partner_copy(i, n, cols).wait_recv()
            both = own0[i, :, cols] + precv[i, :, cols].astype(F32)
            own0[i, :, cols] = both
            xsend[i, :, cols] = both.astype(BF16)
            for k in range(1, n_x):
                chip_copy(i, k, n, cols).start()

    attend_ahead(0)
    finish_halo(0, early, 1)
    wo_load.wait()
    attend_rest(0)
    first_partner(0)
    first_own(0)
    first_sends(0)
    make_queries(0, seg_rows(last - 1))
    second_loads = [
        load(2, w_key.at[1], kv_part(1, 0)),
        load(3, w_value.at[1], kv_part(1, 1)),
        load(8, w_query.at[1], wq.at[1]),
        load(9, w_out.at[1], wo.at[1]),
    ]
    finish_halo(0, late, 0)
    attend(0, last - 1)
    first_partner(1)
    first_own(1)
    make_queries(0, pl.ds(0, (last - 1) * SEG))
    build_edge(0)
    first_sends(1)

    def first_round(i, carry):
        attend(0, last - i)
        first_partner(i)

        @pl.when(i > 2)
        def _():
            first_sends(i - 1)

        first_own(i)
        return carry

    lax.fori_loop(2, segs, first_round, 0)
    first_sends(last)

    def gather_rows(i, seg):
        rows = seg_rows(seg)
        total = own0[i]
        for k in range(1, n_x):
            for n, cols in pieces_of(i):
                chip_copy(i, k, n, cols).wait_recv()
            total = total + xrecv[k - 1, i].astype(F32)
        mine = (cur0[rows, my_half].astype(F32) + total).astype(BF16)
        cur1[rows, my_half] = mine
        rows_copy(i, seg).start()
        squares = half_rows(seg, my_half)
        return squares, half_dot(1, rows, my_half)

    def half_rows(seg, half):
        rows = seg_rows(seg)
        x = cur1[rows, half].astype(F32)
        gained[rows, half] = (x * attn_gain[1:2, half]).astype(BF16)
        return row_squares(x)

    their_start = (1 - my_part) * half_width
    their_half = pl.ds(pl.multiple_of(their_start, 128), half_width)
    quarters = [
        pl.ds(pl.multiple_of(their_start + n * (half_width // 2), 128), half_width // 2)
        for n in range(2)
    ]

    def second_keys(i, seg, squares, flat):
        rows = seg_rows(seg)
        rows_copy(i, seg).wait_recv()
        row_scales = row_scale(squares + half_rows(seg, their_half), width)
        scales[rows, :] = row_scales
        row_scales = widen(row_scales, 2 * kv_width)
        flat = flat * row_scales
        for part in quarters:
            flat = flat + half_dot(1, rows, part) * row_scales
        keys, values = split_keys(1, flat)
        pair_made[1, rows, :] = jnp.concatenate([keys, values], axis=1)
        start_halo(1, rows, 2 + seg)
        put_dup(keys, values, pl.ds(pl.multiple_of(row_count + seg * SEG, SEG), SEG))

    send(psend, precv, ps_sem.at[0], pr_sem.at[0], partner).wait_send()
    for copy in second_loads:
        copy.wait()
    begun = gather_rows(0, last)
    build_bias(1)
    build_edge(1)
    end_halo(0)
    second_keys(0, last, *begun)

    def second_round(i, carry):
        begun = gather_rows(i, last - i)
        make_queries(1, seg_rows(segs - i))
        second_keys(i, last - i, *begun)
        return carry

    lax.fori_loop(1, last, second_round, 0)
    begun = gather_rows(last, 0)
    make_queries(1, seg_rows(1))
    attend_ahead(1)
    finish_halo(1, seg_rows(last), 2 + last)
    second_keys(last, 0, *begun)

    groups = tuple(pl.ds(seg * SEG, SEG) for seg in reversed(range(segs)))

    def near(g, k):
        return g if k == 1 else segs + 1 + (k - 2) * segs + g

    head = last * SEG
    summed_rows = (pl.ds(head + DIRECT, SEG - DIRECT),) + groups[1:]
    beyond = pl.ds(DIRECT, row_count - DIRECT)

    def partner_copy1(g, k):
        rows = summed_rows[g]
        return send(
            psend1.at[k, rows], precv1.at[k, rows], ps_sem.at[k], pr_sem.at[near(g, k)], partner
        )

    def chip_copy1(g, k):
        rows = summed_rows[g]
        return send(
            xsend1.at[k - 1, rows],
            xrecv1.at[k - 1, rows],
            xs_sem.at[k - 1],
            xr1_sem.at[k - 1, g],
            peer(k),
        )

    def direct_copy(k, n):
        return send(
            dsend.at[k - 1, n],
            drecv.at[k - 1, n],
            ds_sem.at[k - 1],
            dr_sem.at[k - 1, n],
            peer(k) if n else far_peer(k),
        )

    far = range(1, n_x)

    def last_partner(g, which):
        for k in which:
            lower = (chip_at(k) * 2 + 1 - core_at(k)) * feat
            made = project_out(1, groups[g], lower, feat).astype(BF16)
            psend1[k, groups[g], :] = made
            if g == 0:
                dsend[k - 1, 0] = made[:DIRECT]
                direct_copy(k, 0).start()
            partner_copy1(g, k).start()

    def last_own(g, which):
        for k in which:
            lower = (chip_at(k) * 2 + core_at(k)) * feat
            made = project_out(1, groups[g], lower, feat)
            own1[k, groups[g], :] = made
            if g == 0:
                dsend[k - 1, 1] = made[:DIRECT].astype(BF16)
                direct_copy(k, 1).start()

    def last_sends(g):
        rows = summed_rows[g]
        for k in far:
            partner_copy1(g, k).wait_recv()
            both = own1[k, rows, :] + precv1[k, rows, :].astype(F32)
            xsend1[k - 1, rows, :] = both.astype(BF16)
            chip_copy1(g, k).start()

    rows_sent = cur1.at[:, my_half]
    send(rows_sent, rows_sent, ps_sem.at[0], cr_sem.at[0], partner).wait_send()
    for k in far:
        send(xsend, xrecv.at[k - 1], xs_sem.at[k - 1], xr_sem.at[k - 1, 0], peer(k)).wait_send()
    attend_rest(1)
    last_partner(0, far)
    last_own(0, far)
    for g in range(1, segs):
        if g == last:
            last_own(g - 1, far)
        finish_halo(1, seg_rows(last - g), 2 + last - g)
        attend(1, last - g)
        if 1 < g < last:
            last_own(g - 1, far)
        if g == last - 1:
            make_queries(1, seg_rows(0))
        last_sends(g - 1)
        last_partner(g, far)
    last_own(last, far)
    last_sends(last)
    near_copy = send(psend1.at[0], precv1.at[0], ps_sem.at[0], pr_sem.at[segs], partner)
    every = pl.ds(0, row_count)
    psend1[0] = project_out(1, every, (chip * 2 + 1 - core) * feat, feat).astype(BF16)
    near_copy.start()
    own1[0] = project_out(1, every, (chip * 2 + core) * feat, feat)
    my_cols = pl.ds(pl.multiple_of(me_tp * feat, 128), feat)
    near_copy.wait_recv()

    def near_total(rows):
        return (
            cur1[rows, my_cols].astype(F32) + own1[0, rows, :] + precv1[0, rows, :].astype(F32)
        )

    rows = pl.ds(head, DIRECT)
    total = near_total(rows)
    for k in range(1, n_x):
        for n in range(2):
            direct_copy(k, n).wait_recv()
            total = total + drecv[k - 1, n].astype(F32)
    out[rows, :] = total.astype(BF16)
    for g in range(len(groups)):
        rows = summed_rows[g]
        total = near_total(rows)
        for k in range(1, n_x):
            chip_copy1(g, k).wait_recv()
            total = total + xrecv1[k - 1, rows, :].astype(F32)
        out[rows, :] = total.astype(BF16)

    near_copy.wait_send()
    for k in range(1, n_x):
        send(
            psend1.at[k, beyond], precv1.at[k, beyond], ps_sem.at[k], pr_sem.at[0], partner
        ).wait_send()
        send(
            xsend1.at[k - 1, beyond],
            xrecv1.at[k - 1, beyond],
            xs_sem.at[k - 1],
            xr1_sem.at[k - 1, 0],
            peer(k),
        ).wait_send()
        send(
            dsend.at[k - 1], drecv.at[k - 1], ds_sem.at[k - 1], dr_sem.at[k - 1, 0], peer(k)
        ).wait_send()
    end_halo(1)


def local(n_sp, n_tp, stream, attn_gain, w_query, w_key, w_value, w_out, query_gain, key_gain, rel_bias):
    row_count, width = stream.shape
    segs = row_count // SEG
    assert row_count == LEFT * SEG and n_tp % 2 == 0
    n_x = n_tp // 2
    feat = width // n_tp
    half_width = width // 2
    q_width = w_query.shape[2]
    kv_width = w_key.shape[2]
    kv_heads = kv_width // HEAD_DIM
    heads = q_width // HEAD_DIM
    group = heads // kv_heads
    others = max(n_x - 1, 1)
    dma = pltpu.SemaphoreType.DMA
    anyw = pl.BlockSpec(memory_space=pltpu.HBM)
    vmem = pl.BlockSpec(memory_space=pltpu.VMEM)
    scratch = [
        pltpu.VMEM(attn_gain.shape, F32),
        pltpu.VMEM(query_gain.shape, F32),
        pltpu.VMEM(key_gain.shape, F32),
        pltpu.VMEM(rel_bias.shape, F32),
        pltpu.VMEM((row_count, width), BF16),
        pltpu.VMEM((row_count, width), BF16),
        pltpu.VMEM((row_count, width), BF16),
        pltpu.VMEM((row_count, 128), F32),
        pltpu.VMEM(w_query.shape, BF16),
        pltpu.VMEM(
            (LAYERS, width, 2 * kv_width) if kv_width % 128 == 0 else (LAYERS, 2, width, kv_width),
            BF16,
        ),
        pltpu.VMEM(w_out.shape, BF16),
        pltpu.VMEM((row_count, q_width), BF16),
        pltpu.VMEM((LAYERS, row_count, 2 * kv_width), BF16),
        pltpu.VMEM((LAYERS, row_count, 2 * kv_width), BF16),
        pltpu.VMEM((kv_heads, 2 * row_count, 128), BF16),
        pltpu.VMEM((kv_heads, 2 * row_count, 256), BF16),
        pltpu.VMEM((LAYERS * heads, LINE), F32),
        pltpu.VMEM((LAYERS, 3, heads * SEG, LINE), F32),
        pltpu.VMEM((kv_heads, group * SEG, 256), F32),
        pltpu.VMEM((row_count, q_width), BF16),
        pltpu.VMEM((segs, SEG, half_width), BF16),
        pltpu.VMEM((segs, SEG, half_width), BF16),
        pltpu.VMEM((segs, SEG, half_width), F32),
        pltpu.VMEM((segs, SEG, half_width), BF16),
        pltpu.VMEM((others, segs, SEG, half_width), BF16),
        pltpu.VMEM((n_x, row_count, feat), BF16),
        pltpu.VMEM((n_x, row_count, feat), BF16),
        pltpu.VMEM((n_x, row_count, feat), F32),
        pltpu.VMEM((others, row_count, feat), BF16),
        pltpu.VMEM((others, row_count, feat), BF16),
        pltpu.VMEM((others, 2, DIRECT, feat), BF16),
        pltpu.VMEM((others, 2, DIRECT, feat), BF16),
        dma((10,)),
        dma((n_x,)), dma((segs + 1 + (others - 1) * segs,)),
        dma((others,)), dma((others, segs + half_width // min(half_width, 512) - 1)),
        dma((segs,)),
        dma((1,)), dma((2 + segs,)),
        dma((others, segs)),
        dma((others,)), dma((others, 2)),
    ]
    return pl.pallas_call(
        functools.partial(body, n_sp, n_tp),
        out_shape=pltpu.VMEM((row_count, feat), BF16),
        in_specs=[anyw] * 9,
        out_specs=vmem,
        scratch_shapes=scratch,
        compiler_params=pltpu.CompilerParams(
            collective_id=0, has_side_effects=True, vmem_limit_bytes=60 * 1024 * 1024
        ),
    )(stream, attn_gain, w_query, w_key, w_value, w_out, query_gain, key_gain, rel_bias)


def solution(mesh):
    return jax.shard_map(
        functools.partial(local, mesh.shape["sp"], mesh.shape["tp"]),
        mesh=mesh,
        in_specs=(
            P("sp", None),
            P(),
            P(None, None, "tp"),
            P(None, None, "tp"),
            P(None, None, "tp"),
            P(None, "tp", None),
            P(),
            P(),
            P(None, "tp", None),
        ),
        out_specs=P("sp", "tp"),
        check_vma=False,
    )
```

```python
import functools

import jax
import jax.numpy as jnp
from jax import lax
from jax.experimental import pallas as pl
from jax.experimental.pallas import tpu as pltpu
from jax.sharding import PartitionSpec as P

HEAD_DIM = 64
SEG = 64
LEFT = 4
CLIP = 128
LAYERS = 2
SPAN = (LEFT + 1) * SEG
LINE = 384
LOG2E = 1.4426950408889634
DIRECT = 32

norm_eps = 1e-06
masked_score = -1e30
F32 = jnp.float32
BF16 = jnp.bfloat16


def seg_rows(seg):
    return pl.ds(pl.multiple_of(seg * SEG, SEG), SEG)


def send(src, dst, send_sem, recv_sem, device):
    return pltpu.make_async_remote_copy(
        src_ref=src,
        dst_ref=dst,
        send_sem=send_sem,
        recv_sem=recv_sem,
        device_id=device,
        device_id_type=pl.DeviceIdType.MESH,
    )


def row_squares(x):
    return jnp.sum(x * x, axis=-1, keepdims=True)


def row_scale(squares, width):
    scale = lax.rsqrt(squares * (1.0 / width) + norm_eps)
    return jnp.broadcast_to(scale, (squares.shape[0], 128))


def widen(scale, width):
    return jnp.concatenate([scale] * -(-width // 128), axis=1)[:, :width]


def head_norm(x, gain_row, scale):
    width = x.shape[1]
    block = min(width, 256)
    row_head = lax.broadcasted_iota(jnp.int32, (block, block), 0) >> 6
    col_head = lax.broadcasted_iota(jnp.int32, (block, block), 1) >> 6
    spread = jnp.where(row_head == col_head, 1.0 / HEAD_DIM, 0.0).astype(BF16)
    gain = jnp.concatenate([gain_row] * (block // HEAD_DIM), axis=1) * scale
    outs = []
    for lower in range(0, width, block):
        part = x[:, lower : lower + block]
        mean = jnp.dot((part * part).astype(BF16), spread, preferred_element_type=F32)
        outs.append((part * lax.rsqrt(mean + norm_eps) * gain).astype(BF16))
    return outs[0] if len(outs) == 1 else jnp.concatenate(outs, axis=1)


def body(
    n_sp, n_tp,
    stream, attn_gain_in, w_query, w_key, w_value, w_out, query_gain_in, key_gain_in, rel_bias_in,
    out,
    attn_gain, query_gain, key_gain, rel_bias,
    cur0, cur1, gained, scales, wq, wkv, wo, queries, pair_made, halo, kdup, vdup, line, bias, ahead, mixed,
    psend, precv, own0, xsend, xrecv,
    psend1, precv1, own1, xsend1, xrecv1, dsend, drecv,
    w_sem, ps_sem, pr_sem, xs_sem, xr_sem, cr_sem, hs_sem, hr_sem, xr1_sem, ds_sem, dr_sem,
):
    row_count, width = cur0.shape
    segs = row_count // SEG
    q_width = wq.shape[2]
    kv_width = w_key.shape[2]
    heads = q_width // HEAD_DIM
    kv_heads = kv_width // HEAD_DIM
    group = heads // kv_heads
    n_x = n_tp // 2
    feat = width // n_tp
    half_width = width // 2
    last = segs - 1
    me_sp = lax.axis_index("sp")
    me_tp = lax.axis_index("tp")
    core = lax.rem(me_tp, 2)
    chip = lax.div(me_tp, 2)
    partner = {"tp": chip * 2 + 1 - core}

    def chip_at(k):
        return lax.rem(chip + k, n_x)

    def core_at(k):
        return lax.rem(core + k, 2)

    def peer(k):
        return {"tp": chip_at(k) * 2 + core_at(k)}

    def far_peer(k):
        return {"tp": chip_at(k) * 2 + 1 - core_at(k)}

    my_part = lax.rem(core + chip, 2)

    barrier = pltpu.get_barrier_semaphore()
    pl.semaphore_signal(barrier, inc=1, device_id=partner, device_id_type=pl.DeviceIdType.MESH)
    for k in range(1, n_x):
        for there in (peer(k), far_peer(k)):
            pl.semaphore_signal(barrier, inc=1, device_id=there, device_id_type=pl.DeviceIdType.MESH)

    @pl.when(me_sp > 0)
    def _():
        pl.semaphore_signal(
            barrier, inc=1, device_id={"sp": me_sp - 1}, device_id_type=pl.DeviceIdType.MESH
        )

    @pl.when(me_sp < n_sp - 1)
    def _():
        pl.semaphore_signal(
            barrier, inc=1, device_id={"sp": me_sp + 1}, device_id_type=pl.DeviceIdType.MESH
        )

    def load(n, src, dst):
        copy = pltpu.make_async_copy(src, dst, w_sem.at[n])
        copy.start()
        return copy

    early = pl.ds(last * SEG, SEG)
    late = pl.ds(0, last * SEG)
    for lower in range(last * SEG, row_count, 16):
        load(0, stream.at[pl.ds(lower, 16)], cur0.at[pl.ds(lower, 16)])
    early_load = pltpu.make_async_copy(stream.at[early], cur0.at[early], w_sem.at[0])
    attn_gain_load = load(1, attn_gain_in, attn_gain)
    joined = kv_width % 128 == 0

    def kv_part(l, n):
        if joined:
            return wkv.at[l, :, pl.ds(n * kv_width, kv_width)]
        return wkv.at[l, n]

    wk_load = load(2, w_key.at[0], kv_part(0, 0))
    wv_load = load(3, w_value.at[0], kv_part(0, 1))
    key_gain_load = load(4, key_gain_in, key_gain)
    late_load = load(5, stream.at[late], cur0.at[late])
    rel_bias_load = load(6, rel_bias_in, rel_bias)
    query_gain_load = load(7, query_gain_in, query_gain)
    wq_load = load(8, w_query.at[0], wq.at[0])
    wo_load = load(9, w_out.at[0], wo.at[0])

    low_half = lax.broadcasted_iota(jnp.int32, (SEG, 128), 1) < HEAD_DIM

    def build_line():
        offset = lax.broadcasted_iota(jnp.int32, (2 * CLIP, LINE), 1)
        distance = jnp.clip(LEFT * SEG + SEG - 1 - offset, -CLIP, CLIP) + CLIP
        match = lax.broadcasted_iota(jnp.int32, (2 * CLIP, LINE), 0) == distance
        onehot = jnp.where(match, 1.0, 0.0).astype(BF16)
        far = (distance[:1] == 2 * CLIP).astype(F32)
        table = jnp.concatenate([rel_bias[l] for l in range(LAYERS)], axis=0)
        near = table[:, : 2 * CLIP]
        high = near.astype(BF16)
        near = near - high.astype(F32)
        middle = near.astype(BF16)
        low = (near - middle.astype(F32)).astype(BF16)
        high, middle, low = (
            jnp.dot(part, onehot, preferred_element_type=F32) for part in (high, middle, low)
        )
        line[...] = (high + middle + low + table[:, 2 * CLIP :] * far) * LOG2E

    def build_bias(l):
        for h in range(heads):
            row = slice(l * heads + h, l * heads + h + 1)
            spread = jnp.broadcast_to(line[row, 128:], (SEG, LINE - 128))
            turned = pltpu.roll(spread, LINE - 128 - (SEG - 1), 1, stride=1, stride_axis=0)
            tiles = [
                jnp.broadcast_to(line[row, :128], (SEG, 128)),
                turned[:, :128],
                jnp.where(low_half, turned[:, 128:], masked_score),
            ]
            top = jnp.maximum(jnp.maximum(tiles[0], tiles[1]), tiles[2])
            peak = jnp.max(top, axis=-1, keepdims=True)
            for n in range(3):
                bias[l, 2, h * SEG : (h + 1) * SEG, n * 128 : (n + 1) * 128] = tiles[n] - peak

    def build_edge(l):
        @pl.when(me_sp == 0)
        def _():
            for h in range(heads):
                rows = slice(h * SEG, (h + 1) * SEG)
                near = bias[l, 2, rows, 256:]
                middle = jnp.where(low_half, masked_score, bias[l, 2, rows, 128:256])
                shut = jnp.full((SEG, 128), masked_score, F32)
                peak = jnp.max(near, axis=-1, keepdims=True)
                bias[l, 0, rows, :128] = shut
                bias[l, 0, rows, 128:256] = shut
                bias[l, 0, rows, 256:] = near - peak
                peak = jnp.maximum(peak, jnp.max(middle, axis=-1, keepdims=True))
                bias[l, 1, rows, :128] = shut
                bias[l, 1, rows, 128:256] = middle - peak
                bias[l, 1, rows, 256:] = near - peak

    for kv in range(kv_heads):
        vdup[kv, :, 128:] = jnp.ones((2 * row_count, 128), BF16)

    def take_rows(l, current, rows):
        x = current[rows, :].astype(F32)
        gained[rows, :] = (x * attn_gain[l : l + 1]).astype(BF16)
        scales[rows, :] = row_scale(row_squares(x), width)

    halves = [pl.ds(n * half_width, half_width) for n in range(2)]

    def half_dot(l, rows, half):
        if joined:
            both = wkv[l, half, :]
        else:
            both = jnp.concatenate([wkv[l, 0, half, :], wkv[l, 1, half, :]], axis=1)
        return jnp.dot(gained[rows, half], both, preferred_element_type=F32)

    def keys_values(l, rows):
        row_scales = widen(scales[rows, :], 2 * kv_width)
        flat = half_dot(l, rows, halves[0]) * row_scales + half_dot(l, rows, halves[1]) * row_scales
        return split_keys(l, flat)

    def split_keys(l, flat):
        keys = head_norm(flat[:, :kv_width], key_gain[l : l + 1], 1.0)
        return keys, flat[:, kv_width:].astype(BF16)

    def make_queries(l, rows):
        flat = jnp.dot(gained[rows, :], wq[l], preferred_element_type=F32)
        queries[rows, :] = head_norm(
            flat * widen(scales[rows, :], q_width),
            query_gain[l : l + 1],
            HEAD_DIM ** (-0.5) * LOG2E,
        )

    def put_dup(keys, values, rows):
        for kv in range(kv_heads):
            cols = slice(kv * HEAD_DIM, (kv + 1) * HEAD_DIM)
            kdup[kv, rows, :] = jnp.concatenate([keys[:, cols]] * 2, axis=1)
            vdup[kv, rows, :128] = jnp.concatenate([values[:, cols]] * 2, axis=1)

    def halo_copy(l, rows, n):
        return send(
            pair_made.at[l, rows],
            halo.at[l, rows],
            hs_sem.at[0],
            hr_sem.at[n],
            {"sp": lax.rem(me_sp + 1, n_sp)},
        )

    def start_halo(l, rows, n, here=True):
        @pl.when(jnp.logical_and(me_sp < n_sp - 1, here))
        def _():
            halo_copy(l, rows, n).start()

    def end_halo(l):
        @pl.when(me_sp < n_sp - 1)
        def _():
            send(
                pair_made.at[l], halo.at[l], hs_sem.at[0], hr_sem.at[0],
                {"sp": lax.rem(me_sp + 1, n_sp)},
            ).wait_send()

    def finish_halo(l, rows, n):
        @pl.when(me_sp > 0)
        def _():
            halo_copy(l, rows, n).wait_recv()
            got = halo[l, rows, :]
            put_dup(got[:, :kv_width], got[:, kv_width:], rows)

    @pl.when(me_sp == 0)
    def _():
        none = jnp.zeros((row_count, 256), BF16)
        for kv in range(kv_heads):
            kdup[kv, 0:row_count, :] = none[:, :128]
            vdup[kv, 0:row_count, :] = none

    def attend_part(l, seg, kv, rows_at, lanes):
        rows = seg_rows(seg)
        stack = []
        for p in range(group // 2):
            lower = (kv * group + 2 * p) * HEAD_DIM
            tile = queries[rows, lower : lower + 128]
            none = jnp.zeros_like(tile)
            stack += [jnp.where(low_half, tile, none), jnp.where(low_half, none, tile)]
        stacked = jnp.concatenate(stack, axis=0)
        scores = lax.dot_general(
            stacked, kdup[kv, rows_at, :], (((1,), (1,)), ((), ())), preferred_element_type=F32
        )
        base = kv * group * SEG
        table = jnp.where(me_sp == 0, jnp.minimum(seg, 2), 2)
        expon = jnp.exp2(scores + bias[l, table, base : base + group * SEG, lanes]).astype(BF16)
        return jnp.dot(expon, vdup[kv, rows_at, :], preferred_element_type=F32)

    def put_mixed(seg, kv, summed):
        rows = seg_rows(seg)
        for p in range(group // 2):
            lower = (kv * group + 2 * p) * HEAD_DIM
            even = summed[2 * p * SEG : (2 * p + 1) * SEG]
            odd = summed[(2 * p + 1) * SEG : (2 * p + 2) * SEG]
            top = jnp.where(low_half, even[:, :128], odd[:, :128])
            under = jnp.where(low_half, even[:, 128:], odd[:, 128:])
            mixed[rows, lower : lower + 128] = (top / under).astype(BF16)

    def attend(l, seg):
        window = pl.ds(pl.multiple_of(seg * SEG, SEG), SPAN)
        for kv in range(kv_heads):
            put_mixed(seg, kv, attend_part(l, seg, kv, window, slice(0, SPAN)))

    late_keys = pl.ds(last * SEG, 2 * SEG)
    early_keys = pl.ds((last + 2) * SEG, SPAN - 2 * SEG)

    def attend_ahead(l):
        for kv in range(kv_heads):
            ahead[kv] = attend_part(l, last, kv, early_keys, slice(2 * SEG, SPAN))

    def attend_rest(l):
        for kv in range(kv_heads):
            rest = attend_part(l, last, kv, late_keys, slice(0, 2 * SEG))
            put_mixed(last, kv, ahead[kv] + rest)

    def project_out(l, rows, lower, size):
        cols = pl.ds(pl.multiple_of(lower, 128), size)
        return jnp.dot(mixed[rows, :], wo[l, :, cols], preferred_element_type=F32)

    def meet():
        at_edge = jnp.logical_or(me_sp == 0, me_sp == n_sp - 1)

        @pl.when(at_edge)
        def _():
            pl.semaphore_wait(barrier, 2 * n_x - 1 + min(n_sp - 1, 1))

        @pl.when(jnp.logical_not(at_edge))
        def _():
            pl.semaphore_wait(barrier, 2 * n_x - 1 + 2)

    early_load.wait()
    attn_gain_load.wait()
    take_rows(0, cur0, early)
    wk_load.wait()
    wv_load.wait()
    key_gain_load.wait()
    keys, values = keys_values(0, early)
    pair_made[0, early, :] = jnp.concatenate([keys, values], axis=1)
    meet()
    start_halo(0, early, 1, core == 0)
    put_dup(keys, values, pl.ds(row_count + last * SEG, SEG))
    late_load.wait()
    take_rows(0, cur0, late)
    start_halo(0, early, 1, core == 1)
    rel_bias_load.wait()
    build_line()
    keys, values = keys_values(0, late)
    pair_made[0, late, :] = jnp.concatenate([keys, values], axis=1)
    start_halo(0, late, 0)
    put_dup(keys, values, pl.ds(row_count, last * SEG))
    query_gain_load.wait()
    wq_load.wait()
    make_queries(0, early)
    build_bias(0)
    out_step = min(half_width, 512)
    whole_piece = pl.ds(0, half_width)
    first_pieces = [pl.ds(lower, out_step) for lower in range(0, half_width, out_step)]

    def pieces_of(i):
        if isinstance(i, int) and i == 0:
            return [(0 if n == 0 else segs + n - 1, cols) for n, cols in enumerate(first_pieces)]
        return [(i, whole_piece)]

    def partner_copy(i, n, cols):
        return send(
            psend.at[i, :, cols], precv.at[i, :, cols], ps_sem.at[0], pr_sem.at[n], partner
        )

    def chip_copy(i, k, n, cols):
        return send(
            xsend.at[i, :, cols],
            xrecv.at[k - 1, i, :, cols],
            xs_sem.at[k - 1],
            xr_sem.at[k - 1, n],
            peer(k),
        )

    my_half = pl.ds(pl.multiple_of(my_part * half_width, 128), half_width)

    def rows_copy(i, seg):
        rows = seg_rows(seg)
        return send(
            cur1.at[rows, my_half], cur1.at[rows, my_half], ps_sem.at[0], cr_sem.at[i], partner
        )

    def first_partner(i):
        for n, cols in pieces_of(i):
            for lower in range(cols.start, cols.start + cols.size, out_step):
                psend[i, :, lower : lower + out_step] = project_out(
                    0, seg_rows(last - i), (1 - my_part) * half_width + lower, out_step
                ).astype(BF16)
            partner_copy(i, n, cols).start()

    def first_own(i):
        for lower in range(0, half_width, out_step):
            own0[i, :, lower : lower + out_step] = project_out(
                0, seg_rows(last - i), my_part * half_width + lower, out_step
            )

    def first_sends(i):
        for n, cols in pieces_of(i):
            partner_copy(i, n, cols).wait_recv()
            both = own0[i, :, cols] + precv[i, :, cols].astype(F32)
            own0[i, :, cols] = both
            xsend[i, :, cols] = both.astype(BF16)
            for k in range(1, n_x):
                chip_copy(i, k, n, cols).start()

    attend_ahead(0)
    finish_halo(0, early, 1)
    wo_load.wait()
    attend_rest(0)
    first_partner(0)
    first_own(0)
    first_sends(0)
    make_queries(0, seg_rows(last - 1))
    second_loads = [
        load(2, w_key.at[1], kv_part(1, 0)),
        load(3, w_value.at[1], kv_part(1, 1)),
        load(8, w_query.at[1], wq.at[1]),
        load(9, w_out.at[1], wo.at[1]),
    ]
    finish_halo(0, late, 0)
    attend(0, last - 1)
    first_partner(1)
    first_own(1)
    make_queries(0, pl.ds(0, (last - 1) * SEG))
    build_edge(0)
    first_sends(1)

    def first_round(i, carry):
        attend(0, last - i)
        first_partner(i)

        @pl.when(i > 2)
        def _():
            first_sends(i - 1)

        first_own(i)
        return carry

    lax.fori_loop(2, segs, first_round, 0)
    first_sends(last)

    def gather_rows(i, seg):
        rows = seg_rows(seg)
        total = own0[i]
        for k in range(1, n_x):
            for n, cols in pieces_of(i):
                chip_copy(i, k, n, cols).wait_recv()
            total = total + xrecv[k - 1, i].astype(F32)
        mine = (cur0[rows, my_half].astype(F32) + total).astype(BF16)
        cur1[rows, my_half] = mine
        rows_copy(i, seg).start()
        squares = half_rows(seg, my_half)
        return squares, half_dot(1, rows, my_half)

    def half_rows(seg, half):
        rows = seg_rows(seg)
        x = cur1[rows, half].astype(F32)
        gained[rows, half] = (x * attn_gain[1:2, half]).astype(BF16)
        return row_squares(x)

    their_start = (1 - my_part) * half_width
    their_half = pl.ds(pl.multiple_of(their_start, 128), half_width)
    quarters = [
        pl.ds(pl.multiple_of(their_start + n * (half_width // 2), 128), half_width // 2)
        for n in range(2)
    ]

    def second_keys(i, seg, squares, flat):
        rows = seg_rows(seg)
        rows_copy(i, seg).wait_recv()
        row_scales = row_scale(squares + half_rows(seg, their_half), width)
        scales[rows, :] = row_scales
        row_scales = widen(row_scales, 2 * kv_width)
        flat = flat * row_scales
        for part in quarters:
            flat = flat + half_dot(1, rows, part) * row_scales
        keys, values = split_keys(1, flat)
        pair_made[1, rows, :] = jnp.concatenate([keys, values], axis=1)
        start_halo(1, rows, 2 + seg)
        put_dup(keys, values, pl.ds(pl.multiple_of(row_count + seg * SEG, SEG), SEG))

    send(psend, precv, ps_sem.at[0], pr_sem.at[0], partner).wait_send()
    for copy in second_loads:
        copy.wait()
    begun = gather_rows(0, last)
    build_bias(1)
    build_edge(1)
    end_halo(0)
    second_keys(0, last, *begun)

    def second_round(i, carry):
        begun = gather_rows(i, last - i)
        make_queries(1, seg_rows(segs - i))
        second_keys(i, last - i, *begun)
        return carry

    lax.fori_loop(1, last, second_round, 0)
    begun = gather_rows(last, 0)
    make_queries(1, seg_rows(1))
    attend_ahead(1)
    finish_halo(1, seg_rows(last), 2 + last)
    second_keys(last, 0, *begun)

    groups = tuple(pl.ds(seg * SEG, SEG) for seg in reversed(range(segs)))

    def near(g, k):
        return g if k == 1 else segs + 1 + (k - 2) * segs + g

    head = last * SEG
    summed_rows = (pl.ds(head + DIRECT, SEG - DIRECT),) + groups[1:]
    beyond = pl.ds(DIRECT, row_count - DIRECT)

    def partner_copy1(g, k):
        rows = summed_rows[g]
        return send(
            psend1.at[k, rows], precv1.at[k, rows], ps_sem.at[k], pr_sem.at[near(g, k)], partner
        )

    def chip_copy1(g, k):
        rows = summed_rows[g]
        return send(
            xsend1.at[k - 1, rows],
            xrecv1.at[k - 1, rows],
            xs_sem.at[k - 1],
            xr1_sem.at[k - 1, g],
            peer(k),
        )

    def direct_copy(k, n):
        return send(
            dsend.at[k - 1, n],
            drecv.at[k - 1, n],
            ds_sem.at[k - 1],
            dr_sem.at[k - 1, n],
            peer(k) if n else far_peer(k),
        )

    far = range(1, n_x)

    def last_partner(g, which):
        for k in which:
            lower = (chip_at(k) * 2 + 1 - core_at(k)) * feat
            made = project_out(1, groups[g], lower, feat).astype(BF16)
            psend1[k, groups[g], :] = made
            if g == 0:
                dsend[k - 1, 0] = made[:DIRECT]
                direct_copy(k, 0).start()
            partner_copy1(g, k).start()

    def last_own(g, which):
        for k in which:
            lower = (chip_at(k) * 2 + core_at(k)) * feat
            made = project_out(1, groups[g], lower, feat)
            own1[k, groups[g], :] = made
            if g == 0:
                dsend[k - 1, 1] = made[:DIRECT].astype(BF16)
                direct_copy(k, 1).start()

    def last_sends(g):
        rows = summed_rows[g]
        for k in far:
            partner_copy1(g, k).wait_recv()
            both = own1[k, rows, :] + precv1[k, rows, :].astype(F32)
            xsend1[k - 1, rows, :] = both.astype(BF16)
            chip_copy1(g, k).start()

    rows_sent = cur1.at[:, my_half]
    send(rows_sent, rows_sent, ps_sem.at[0], cr_sem.at[0], partner).wait_send()
    for k in far:
        send(xsend, xrecv.at[k - 1], xs_sem.at[k - 1], xr_sem.at[k - 1, 0], peer(k)).wait_send()
    attend_rest(1)
    last_partner(0, far)
    last_own(0, far)
    for g in range(1, segs):
        if g == last:
            last_own(g - 1, far)
        finish_halo(1, seg_rows(last - g), 2 + last - g)
        attend(1, last - g)
        if 1 < g < last:
            last_own(g - 1, far)
        if g == last - 1:
            make_queries(1, seg_rows(0))
        last_sends(g - 1)
        last_partner(g, far)
    last_own(last, far)
    last_sends(last)
    near_copy = send(psend1.at[0], precv1.at[0], ps_sem.at[0], pr_sem.at[segs], partner)
    every = pl.ds(0, row_count)
    psend1[0] = project_out(1, every, (chip * 2 + 1 - core) * feat, feat).astype(BF16)
    near_copy.start()
    own1[0] = project_out(1, every, (chip * 2 + core) * feat, feat)
    my_cols = pl.ds(pl.multiple_of(me_tp * feat, 128), feat)
    near_copy.wait_recv()

    def near_total(rows):
        return (
            cur1[rows, my_cols].astype(F32) + own1[0, rows, :] + precv1[0, rows, :].astype(F32)
        )

    rows = pl.ds(head, DIRECT)
    total = near_total(rows)
    for k in range(1, n_x):
        for n in range(2):
            direct_copy(k, n).wait_recv()
            total = total + drecv[k - 1, n].astype(F32)
    out[rows, :] = total.astype(BF16)
    for g in range(len(groups)):
        rows = summed_rows[g]
        total = near_total(rows)
        for k in range(1, n_x):
            chip_copy1(g, k).wait_recv()
            total = total + xrecv1[k - 1, rows, :].astype(F32)
        out[rows, :] = total.astype(BF16)

    near_copy.wait_send()
    for k in range(1, n_x):
        send(
            psend1.at[k, beyond], precv1.at[k, beyond], ps_sem.at[k], pr_sem.at[0], partner
        ).wait_send()
        send(
            xsend1.at[k - 1, beyond],
            xrecv1.at[k - 1, beyond],
            xs_sem.at[k - 1],
            xr1_sem.at[k - 1, 0],
            peer(k),
        ).wait_send()
        send(
            dsend.at[k - 1], drecv.at[k - 1], ds_sem.at[k - 1], dr_sem.at[k - 1, 0], peer(k)
        ).wait_send()
    end_halo(1)


def local(n_sp, n_tp, stream, attn_gain, w_query, w_key, w_value, w_out, query_gain, key_gain, rel_bias):
    row_count, width = stream.shape
    segs = row_count // SEG
    assert row_count == LEFT * SEG and n_tp % 2 == 0
    n_x = n_tp // 2
    feat = width // n_tp
    half_width = width // 2
    q_width = w_query.shape[2]
    kv_width = w_key.shape[2]
    kv_heads = kv_width // HEAD_DIM
    heads = q_width // HEAD_DIM
    group = heads // kv_heads
    others = max(n_x - 1, 1)
    dma = pltpu.SemaphoreType.DMA
    anyw = pl.BlockSpec(memory_space=pltpu.HBM)
    vmem = pl.BlockSpec(memory_space=pltpu.VMEM)
    scratch = [
        pltpu.VMEM(attn_gain.shape, F32),
        pltpu.VMEM(query_gain.shape, F32),
        pltpu.VMEM(key_gain.shape, F32),
        pltpu.VMEM(rel_bias.shape, F32),
        pltpu.VMEM((row_count, width), BF16),
        pltpu.VMEM((row_count, width), BF16),
        pltpu.VMEM((row_count, width), BF16),
        pltpu.VMEM((row_count, 128), F32),
        pltpu.VMEM(w_query.shape, BF16),
        pltpu.VMEM(
            (LAYERS, width, 2 * kv_width) if kv_width % 128 == 0 else (LAYERS, 2, width, kv_width),
            BF16,
        ),
        pltpu.VMEM(w_out.shape, BF16),
        pltpu.VMEM((row_count, q_width), BF16),
        pltpu.VMEM((LAYERS, row_count, 2 * kv_width), BF16),
        pltpu.VMEM((LAYERS, row_count, 2 * kv_width), BF16),
        pltpu.VMEM((kv_heads, 2 * row_count, 128), BF16),
        pltpu.VMEM((kv_heads, 2 * row_count, 256), BF16),
        pltpu.VMEM((LAYERS * heads, LINE), F32),
        pltpu.VMEM((LAYERS, 3, heads * SEG, LINE), F32),
        pltpu.VMEM((kv_heads, group * SEG, 256), F32),
        pltpu.VMEM((row_count, q_width), BF16),
        pltpu.VMEM((segs, SEG, half_width), BF16),
        pltpu.VMEM((segs, SEG, half_width), BF16),
        pltpu.VMEM((segs, SEG, half_width), F32),
        pltpu.VMEM((segs, SEG, half_width), BF16),
        pltpu.VMEM((others, segs, SEG, half_width), BF16),
        pltpu.VMEM((n_x, row_count, feat), BF16),
        pltpu.VMEM((n_x, row_count, feat), BF16),
        pltpu.VMEM((n_x, row_count, feat), F32),
        pltpu.VMEM((others, row_count, feat), BF16),
        pltpu.VMEM((others, row_count, feat), BF16),
        pltpu.VMEM((others, 2, DIRECT, feat), BF16),
        pltpu.VMEM((others, 2, DIRECT, feat), BF16),
        dma((10,)),
        dma((n_x,)), dma((segs + 1 + (others - 1) * segs,)),
        dma((others,)), dma((others, segs + half_width // min(half_width, 512) - 1)),
        dma((segs,)),
        dma((1,)), dma((2 + segs,)),
        dma((others, segs)),
        dma((others,)), dma((others, 2)),
    ]
    return pl.pallas_call(
        functools.partial(body, n_sp, n_tp),
        out_shape=pltpu.VMEM((row_count, feat), BF16),
        in_specs=[anyw] * 9,
        out_specs=vmem,
        scratch_shapes=scratch,
        compiler_params=pltpu.CompilerParams(
            collective_id=0, has_side_effects=True, vmem_limit_bytes=60 * 1024 * 1024
        ),
    )(stream, attn_gain, w_query, w_key, w_value, w_out, query_gain, key_gain, rel_bias)


def solution(mesh):
    return jax.shard_map(
        functools.partial(local, mesh.shape["sp"], mesh.shape["tp"]),
        mesh=mesh,
        in_specs=(
            P("sp", None),
            P(),
            P(None, None, "tp"),
            P(None, None, "tp"),
            P(None, None, "tp"),
            P(None, "tp", None),
            P(),
            P(),
            P(None, "tp", None),
        ),
        out_specs=P("sp", "tp"),
        check_vma=False,
    )
```
